32 devices in a mesh: grp: 2 (over x), tp: 4 (over y, core), dp: 4 (over z).
Axes of the slice: x: 2, y: 2, z: 4, core: 2. Of those that a mesh axis runs over, the one named last changes fastest.
Arguments:
- tokens: bfloat16 [64, 4096], P(('grp', 'tp'), 'dp'), parts along dimension 0, may hold values from -45 to 45
- w_in: bfloat16 [2, 2, 4096, 8192], P(None, None, 'dp', 'tp'), may hold values from -0.09375 to 0.09375
- w_vec: bfloat16 [2, 2, 4096, 2048], P(None, None, 'dp', 'tp'), may hold values from -0.09375 to 0.09375
- w_step: bfloat16 [2, 4096, 128], P(None, 'dp'), may hold values from -0.09375 to 0.09375
- conv_weight: bfloat16 [2, 4, 8192], P(None, None, 'tp'), may hold values from -3 to 3
- conv_vec: bfloat16 [2, 2, 4, 2048], P(None, None, None, 'tp'), may hold values from -3 to 3
- conv_state: bfloat16 [2, 64, 3, 8192], P(None, ('grp', 'dp'), None, 'tp'), parts along dimension 1, may hold values from -6 to 6
- vec_state: bfloat16 [2, 2, 64, 3, 2048], P(None, None, ('grp', 'dp'), None, 'tp'), parts along dimension 2, may hold values from -6 to 6
- ssm_state: float32 [2, 64, 128, 64, 128], P(None, ('grp', 'dp'), 'tp'), parts along dimension 1, may hold values from -4 to 4
- step_bias: float32 [2, 128], P(None, 'tp'), may hold values from -1.5 to 1
- decay_log: float32 [2, 128], P(None, 'tp'), may hold values from -4 to 1
- skip_gain: float32 [2, 128], P(None, 'tp'), may hold values from 0.5 to 3
- mix_gain: bfloat16 [2, 4096], P(None, 'dp'), may hold values from 0.099609375 to 1.8984375
- out_gain: bfloat16 [2, 8192], P(None, 'tp'), may hold values from 0.099609375 to 1.8984375
- w_out: bfloat16 [2, 8192, 4096], P(None, 'tp', 'dp'), may hold values from -0.0625 to 0.0625
Outputs:
- new_tokens: bfloat16 [64, 4096], P(('grp', 'tp'), 'dp'), parts along dimension 0
- new_conv: bfloat16 [2, 64, 3, 8192], P(None, ('grp', 'dp'), None, 'tp'), parts along dimension 1
- new_vec: bfloat16 [2, 2, 64, 3, 2048], P(None, None, ('grp', 'dp'), None, 'tp'), parts along dimension 2
- new_ssm: float32 [2, 64, 128, 64, 128], P(None, ('grp', 'dp'), 'tp'), parts along dimension 1
The draws below stay inside these ranges and needn't reach their ends.
There are 2 independent parts, one for each index of `grp`. The reference program is written for one: setup_inputs(seed, part) draws one part's arguments, and reference() takes and returns one part's arrays. A program takes and returns all parts, laid end to end along the dimension named above; an argument that names none is the same for every part. Nothing has to cross between parts.
All inputs are finite; a program needn't handle non-finite values.
Results may differ from the reference program's by a relative error of at most 0.023.
Values may be sent and summed in bfloat16 or wider, within the bound.
A program may use at most 128 MiB of HBM per device.

```python
import jax
import jax.numpy as jnp
from jax import lax

MODEL_WIDTH = 4096
HEAD_COUNT = 128
HEAD_DIM = 64
STATE_DIM = 128
GROUP_COUNT = 16
CONV_TAPS = 4
LAYER_COUNT = 2
INNER_WIDTH = 8192
VEC_WIDTH = 2048
BATCH_SEQS = 32


def draw_tokens(key, part):
    base_key = jax.random.fold_in(key, 17)
    key_base, key_row = jax.random.split(base_key, 2)
    columns = jnp.exp(jnp.linspace(jnp.log(0.4), jnp.log(2.4), MODEL_WIDTH)).astype(jnp.float32)
    row_scale = jnp.exp(jax.random.uniform(key_row, (BATCH_SEQS, 1), jnp.float32, 0.0, jnp.log(10.0)))
    base = jnp.clip(jax.random.normal(key_base, (BATCH_SEQS, MODEL_WIDTH), jnp.float32), -6.0, 6.0)
    return (0.3 * base * columns[None, :] * row_scale).astype(jnp.bfloat16)


def levels(rng, extent, shards, low, largest):
    factor_of = 1.0
    for axis_at, parts in shards:
        heights = jax.random.uniform(jax.random.fold_in(jax.random.fold_in(rng, 6), axis_at), (parts,), jnp.float32, low / len(shards), largest / len(shards))
        factor_of = factor_of * jnp.repeat(jnp.exp(heights), extent[axis_at] // parts).reshape((-1,) + (1,) * (len(extent) - 1 - axis_at))
    return factor_of


def bell_draw(rng, extent, width, bound, cuts=(), dtype=jnp.bfloat16):
    values = width * jax.random.normal(rng, extent, jnp.float32)
    if cuts:
        values = values * levels(rng, extent, cuts, -0.22, 0.18)
    return jnp.clip(values, -bound, bound).astype(dtype)


def setup_inputs(seed: int = 0, part: int = 0) -> dict:
    key_of = jax.random.split(jax.random.key(seed), 16)
    part_splits = jax.random.split(jax.random.fold_in(key_of[15], part), 16)
    return {
        "tokens": draw_tokens(jax.random.fold_in(jax.random.fold_in(key_of[15], part), 71), part),
        "w_in": bell_draw(key_of[1], (LAYER_COUNT, 2, MODEL_WIDTH, INNER_WIDTH), MODEL_WIDTH ** -0.5, 0.09375, ((2, 4), (3, 4))),
        "w_vec": bell_draw(key_of[2], (LAYER_COUNT, 2, MODEL_WIDTH, VEC_WIDTH), MODEL_WIDTH ** -0.5, 0.09375, ((2, 4), (3, 4))),
        "w_step": bell_draw(key_of[3], (LAYER_COUNT, MODEL_WIDTH, HEAD_COUNT), MODEL_WIDTH ** -0.5, 0.09375, ((1, 4),)),
        "conv_weight": bell_draw(key_of[4], (LAYER_COUNT, CONV_TAPS, INNER_WIDTH), 0.5, 3.0, ((2, 4),)),
        "conv_vec": bell_draw(key_of[5], (LAYER_COUNT, 2, CONV_TAPS, VEC_WIDTH), 0.5, 3.0, ((3, 4),)),
        "conv_state": bell_draw(part_splits[6], (LAYER_COUNT, BATCH_SEQS, CONV_TAPS - 1, INNER_WIDTH), 1.0, 6.0, ((1, 4), (3, 4))),
        "vec_state": bell_draw(part_splits[7], (LAYER_COUNT, 2, BATCH_SEQS, CONV_TAPS - 1, VEC_WIDTH), 1.0, 6.0, ((2, 4), (4, 4))),
        "ssm_state": bell_draw(part_splits[8], (LAYER_COUNT, BATCH_SEQS, HEAD_COUNT, HEAD_DIM, STATE_DIM), 0.5, 4.0, ((1, 4), (2, 4)), jnp.float32),
        "step_bias": jnp.clip(-1.5 + 2.5 * jax.random.uniform(key_of[9], (LAYER_COUNT, HEAD_COUNT), jnp.float32) ** levels(key_of[9], (LAYER_COUNT, HEAD_COUNT), ((1, 4),), -0.2, 0.2), -1.5, 1.0),
        "decay_log": jnp.clip(-4.0 + 5.0 * jax.random.uniform(key_of[10], (LAYER_COUNT, HEAD_COUNT), jnp.float32) ** levels(key_of[10], (LAYER_COUNT, HEAD_COUNT), ((1, 4),), -0.2, 0.2), -4.0, 1.0),
        "skip_gain": jnp.clip(0.5 + 2.5 * jax.random.uniform(key_of[11], (LAYER_COUNT, HEAD_COUNT), jnp.float32) ** levels(key_of[11], (LAYER_COUNT, HEAD_COUNT), ((1, 4),), -0.2, 0.2), 0.5, 3.0),
        "mix_gain": jnp.clip(1.0 + 0.18 * jax.random.normal(key_of[12], (LAYER_COUNT, MODEL_WIDTH), jnp.float32), 0.099609375, 1.8984375).astype(jnp.bfloat16),
        "out_gain": jnp.clip(1.0 + 0.18 * jax.random.normal(key_of[13], (LAYER_COUNT, INNER_WIDTH), jnp.float32), 0.099609375, 1.8984375).astype(jnp.bfloat16),
        "w_out": bell_draw(key_of[14], (LAYER_COUNT, INNER_WIDTH, MODEL_WIDTH), INNER_WIDTH ** -0.5, 0.0625, ((1, 4), (2, 4))),
    }


EPS = 1e-06

def mixer(current, layer, w_in, w_vec, w_step, conv_weight, conv_vec, conv_state, vec_state, ssm_state, step_bias, decay_log, skip_gain, mix_gain, out_gain, w_out):
    batch = current.shape[0]
    xf = current.astype(jnp.float32)
    scale = lax.rsqrt(lax.optimization_barrier(jnp.mean(xf * xf, axis=1)) + EPS)
    scaled_in = (xf * mix_gain[layer].astype(jnp.float32)).astype(jnp.bfloat16)
    proj = jnp.einsum('bd,rdc->brc', scaled_in.astype(jnp.float32), w_in[layer].astype(jnp.float32))
    proj = (proj * scale[:, None, None]).astype(jnp.bfloat16)
    vecs = jnp.einsum('bd,rdc->brc', scaled_in.astype(jnp.float32), w_vec[layer].astype(jnp.float32))
    vecs = (vecs * scale[:, None, None]).astype(jnp.bfloat16)
    step_raw = jnp.dot(scaled_in, w_step[layer], preferred_element_type=jnp.float32) * scale[:, None]
    window = jnp.concatenate([conv_state[layer], proj[:, 1][:, None, :]], axis=1)
    new_conv = window[:, 1:, :]
    values_sum = lax.optimization_barrier(jnp.sum(window.astype(jnp.float32) * conv_weight[layer].astype(jnp.float32)[None, :, :], axis=1))
    fresh = jnp.transpose(vecs, (1, 0, 2))[:, :, None, :]
    vec_window = jnp.concatenate([vec_state[layer], fresh], axis=2)
    new_vec = vec_window[:, :, 1:, :]
    vec_sum = lax.optimization_barrier(jnp.sum(vec_window.astype(jnp.float32) * conv_vec[layer].astype(jnp.float32)[:, None, :, :], axis=2))
    values = jax.nn.silu(values_sum).reshape(batch, HEAD_COUNT, HEAD_DIM)
    vec_act = jax.nn.silu(vec_sum)
    repeat = HEAD_COUNT // GROUP_COUNT
    in_vec = jnp.repeat(vec_act[0].reshape(batch, GROUP_COUNT, STATE_DIM), repeat, axis=1)
    out_vec = jnp.repeat(vec_act[1].reshape(batch, GROUP_COUNT, STATE_DIM), repeat, axis=1)
    step = jax.nn.softplus(step_raw + step_bias[layer][None, :])
    decay = jnp.exp(-step * jnp.exp(decay_log[layer])[None, :])
    state = decay[:, :, None, None] * ssm_state[layer] + (step[:, :, None] * values)[..., None] * in_vec[:, :, None, :]
    read = jnp.einsum('bhpn,bhn->bhp', state, out_vec) + skip_gain[layer][None, :, None] * values
    mixed = read.reshape(batch, INNER_WIDTH) * jax.nn.silu(proj[:, 0].astype(jnp.float32))
    grouped = mixed.reshape(batch, GROUP_COUNT, INNER_WIDTH // GROUP_COUNT)
    grouped = grouped * lax.rsqrt(lax.optimization_barrier(jnp.mean(grouped * grouped, axis=2, keepdims=True)) + EPS)
    normed = (grouped.reshape(batch, INNER_WIDTH) * out_gain[layer].astype(jnp.float32)).astype(jnp.bfloat16)
    result = (xf + jnp.dot(normed, w_out[layer], preferred_element_type=jnp.float32)).astype(jnp.bfloat16)
    return (result, new_conv, new_vec, state)

def reference(tokens, w_in, w_vec, w_step, conv_weight, conv_vec, conv_state, vec_state, ssm_state, step_bias, decay_log, skip_gain, mix_gain, out_gain, w_out):
    current = tokens
    convs = []
    vec_rows = []
    states = []
    for layer in range(LAYER_COUNT):
        current, conv_next, vec_next, state_next = mixer(current, layer, w_in, w_vec, w_step, conv_weight, conv_vec, conv_state, vec_state, ssm_state, step_bias, decay_log, skip_gain, mix_gain, out_gain, w_out)
        convs.append(conv_next)
        vec_rows.append(vec_next)
        states.append(state_next)
    return (current, jnp.stack(convs), jnp.stack(vec_rows), jnp.stack(states))
```

```python
import functools

import jax
import jax.numpy as jnp
from jax import lax
from jax.experimental import pallas as pl
from jax.experimental.pallas import tpu as pltpu
from jax.sharding import PartitionSpec as P

MODEL_WIDTH = 4096
HEAD_DIM = 64
STATE_DIM = 128
LANES = 128
LAYER_COUNT = 2

EPS = 1e-06
F32 = jnp.float32
BF16 = jnp.bfloat16


def remote(src, dst, send_sem, recv_sem, axis, target):
    return pltpu.make_async_remote_copy(
        src_ref=src,
        dst_ref=dst,
        send_sem=send_sem,
        recv_sem=recv_sem,
        device_id={axis: target},
        device_id_type=pl.DeviceIdType.MESH,
    )


def greet(sizes):
    barrier = pltpu.get_barrier_semaphore()
    count = 0
    for axis, n in sizes:
        me = lax.axis_index(axis)
        for k in range(1, n):
            pl.semaphore_signal(
                barrier,
                inc=1,
                device_id={axis: lax.rem(me + k, n)},
                device_id_type=pl.DeviceIdType.MESH,
            )
            count += 1
    pl.semaphore_wait(barrier, count)


def silu(v):
    return v / (1.0 + jnp.exp(-v))


def softplus(v):
    return jnp.maximum(v, 0.0) + jnp.log1p(jnp.exp(-jnp.abs(v)))


def expand(per_head, at, rows):
    per = LANES // HEAD_DIM
    lane = lax.broadcasted_iota(jnp.int32, (rows, LANES), 1)
    out = jnp.broadcast_to(per_head[:, at : at + 1], (rows, LANES))
    for j in range(1, per):
        other = jnp.broadcast_to(per_head[:, at + j : at + j + 1], (rows, LANES))
        out = jnp.where(lane >= j * HEAD_DIM, other, out)
    return out


def mixer_kernel(
    ntp, ndp,
    x_ref, gain_hbm, w_step_hbm, w_in_hbm, w_vec_hbm, w_out_hbm, conv_w_hbm, conv_v_hbm,
    conv_hbm, vec_hbm, ssm_hbm, bias_hbm, decay_hbm, skip_hbm, out_gain_hbm,
    tok_ref, new_conv, new_vec, ssm_ref,
    w_step, w_in, w_vec, w_out, gain, conv_w, conv_v, conv_s, vec_s, bias, decay_log, skip, out_gain,
    landed, lhs_buf, send_small, recv_small, send_proj, recv_proj,
    ins_buf, outs_buf, read_buf, drive_pad, drive_t, decay_pad, decay_t,
    held, lhs_out, part_out, parts_in, rows_buf, send_out, recv_out,
    small_sem, weight_sem, ssm_sem, ssem_x, rsem_x, ssem_s, rsem_s, ssem_p, rsem_p,
    ssem_n, rsem_n, ssem_o, rsem_o, ssem_f, rsem_f,
):
    rows_t, width = x_ref.shape
    batch = rows_t * ntp
    rows_d = batch // ndp
    cols = w_in.shape[3]
    vcols = w_vec.shape[3]
    heads = w_step.shape[2]
    local_heads = ssm_ref.shape[2]
    groups = vcols // STATE_DIM
    span = cols // groups
    group_heads = local_heads // groups
    block = min(cols, 1024)
    blocks = cols // block
    tp = lax.axis_index("tp")
    dp = lax.axis_index("dp")
    pending = []

    def load(src, dst, sem):
        copy = pltpu.make_async_copy(src, dst, sem)
        copy.start()
        return copy

    def load_weights(layer):
        vec = load(w_vec_hbm.at[layer], w_vec.at[layer], weight_sem.at[layer, 0])
        step = load(w_step_hbm.at[layer], w_step.at[layer], weight_sem.at[layer, 1])
        return vec, step, [
            load(w_in_hbm.at[layer, role], w_in.at[layer, role], weight_sem.at[layer, 2 + role])
            for role in (1, 0)
        ]

    smalls = [
        load(src, dst, small_sem.at[i])
        for i, (src, dst) in enumerate(
            (
                (gain_hbm, gain), (conv_w_hbm, conv_w), (conv_v_hbm, conv_v),
                (conv_hbm, conv_s), (vec_hbm, vec_s), (bias_hbm, bias),
                (decay_hbm, decay_log), (skip_hbm, skip), (out_gain_hbm, out_gain),
            )
        )
    ]
    weights = [load_weights(0)]
    greet((("tp", ntp), ("dp", ndp)))
    gathers = []
    for k in range(1, ntp):
        copy = remote(
            x_ref, landed.at[tp], ssem_x.at[k], rsem_x.at[k], "tp", lax.rem(tp + k, ntp)
        )
        copy.start()
        gathers.append(copy)
    landed[tp] = x_ref[...]
    drive_pad[...] = jnp.zeros_like(drive_pad)
    decay_pad[...] = jnp.zeros_like(decay_pad)
    for copy in smalls:
        copy.wait()
    for copy in gathers:
        copy.wait()
    out_loads = []
    state_loads = []

    def project(layer, rows):
        scale_row = gain[...].astype(F32)[layer : layer + 1]
        squares = []
        for i in range(ntp):
            part = rows(i)
            squares.append(jnp.sum(part * part, axis=1, keepdims=True))
            lhs_buf[i * rows_t : (i + 1) * rows_t, :] = part * scale_row
        squares = jnp.concatenate(squares, axis=0)
        lhs = lhs_buf[...].astype(BF16)
        load_vec, load_step, load_in = weights[layer]

        def put(target, at, acc):
            for p in range(ndp):
                target[p, :, at : at + acc.shape[1]] = acc[p * rows_d : (p + 1) * rows_d].astype(
                    BF16
                )

        def deal(target, landing, ssem, rsem):
            copies = []
            for k in range(ndp - 1, 0, -1):
                peer = lax.rem(dp + k, ndp)
                copy = remote(target.at[peer], landing.at[k], ssem.at[k], rsem.at[k], "dp", peer)
                copy.start()
                copies.append(copy)
            pending.extend(copies)
            return copies

        load_step.wait()
        load_vec.wait()
        small = jnp.dot(lhs, w_step[layer], preferred_element_type=F32)
        small = pltpu.roll(small, lax.rem(heads - tp * local_heads, heads), 1)
        lane = lax.broadcasted_iota(jnp.int32, small.shape, 1)
        small = jnp.where(lane == local_heads, jnp.broadcast_to(squares, small.shape), small)
        put(send_small.at[layer], 2 * vcols, small)
        for role in range(2):
            put(
                send_small.at[layer], role * vcols,
                jnp.dot(lhs, w_vec[layer, role], preferred_element_type=F32),
            )
        flights = [
            deal(send_small.at[layer], recv_small.at[layer], ssem_s.at[layer], rsem_s.at[layer])
        ]
        for j, role in enumerate((1, 0)):
            load_in[j].wait()
            for b in range(blocks):
                c = j * blocks + b
                acc = jnp.dot(
                    lhs, w_in[layer, role, :, b * block : (b + 1) * block],
                    preferred_element_type=F32,
                )
                put(send_proj.at[layer, c], 0, acc)
                flights.append(
                    deal(
                        send_proj.at[layer, c], recv_proj.at[layer, c],
                        ssem_p.at[layer, c], rsem_p.at[layer, c],
                    )
                )
        return flights

    def total(mine, others):
        acc = mine[dp].astype(F32)
        for k in range(1, ndp):
            acc = acc + others[k].astype(F32)
        return acc

    def head_step(layer, flights):
        for copy in flights[0]:
            copy.wait_recv()
        small = total(send_small.at[layer], recv_small.at[layer])
        own_sq = small[:, 2 * vcols + local_heads : 2 * vcols + local_heads + 1]
        scale = lax.rsqrt(own_sq * (1.0 / MODEL_WIDTH) + EPS)
        taps_v = conv_v[layer].astype(F32)
        acts = []
        for role in range(2):
            fresh = (small[:, role * vcols : (role + 1) * vcols] * scale).astype(BF16)
            acc = fresh.astype(F32) * taps_v[role, 3:4]
            for i in range(3):
                acc = acc + vec_s[layer, role, i].astype(F32) * taps_v[role, i : i + 1]
            new_vec[layer, role, 0] = vec_s[layer, role, 1]
            new_vec[layer, role, 1] = vec_s[layer, role, 2]
            new_vec[layer, role, 2] = fresh
            acts.append(silu(acc))
        in_vec, out_vec = acts
        step = softplus(
            small[:, 2 * vcols : 2 * vcols + local_heads] * scale + bias[layer : layer + 1]
        )
        decay = jnp.exp(-step * jnp.exp(decay_log[layer : layer + 1]))
        decay_pad[0:rows_d, 0:local_heads] = decay
        decay_t[...] = jnp.transpose(decay_pad[...])
        state_loads[layer].wait()
        row = lax.broadcasted_iota(jnp.int32, (rows_d, STATE_DIM), 0)
        skips = jnp.broadcast_to(skip[layer : layer + 1], (rows_d, local_heads))
        for g in range(groups):
            ins_buf[g] = in_vec[:, g * STATE_DIM : (g + 1) * STATE_DIM]
            outs_buf[g] = out_vec[:, g * STATE_DIM : (g + 1) * STATE_DIM]
            out_g = outs_buf[g]
            acc = jnp.zeros((rows_d, span), F32)
            for r in range(rows_d):
                mine = jnp.where(row == r, out_g, 0.0)
                state = ssm_ref[layer, r, g * group_heads : (g + 1) * group_heads]
                acc = acc + lax.dot_general(
                    mine, state.reshape(span, STATE_DIM), (((1,), (1,)), ((), ())),
                    preferred_element_type=F32,
                )
            read_buf[:, g * span : (g + 1) * span] = acc
        taps = conv_w[layer].astype(F32)
        for b in range(blocks):
            for copy in flights[1 + b]:
                copy.wait_recv()
            cut = slice(b * block, (b + 1) * block)
            fresh = (total(send_proj.at[layer, b], recv_proj.at[layer, b]) * scale).astype(BF16)
            acc = fresh.astype(F32) * taps[3:4, cut]
            for i in range(3):
                acc = acc + conv_s[layer, i, :, cut].astype(F32) * taps[i : i + 1, cut]
            new_conv[layer, 0, :, cut] = conv_s[layer, 1, :, cut]
            new_conv[layer, 1, :, cut] = conv_s[layer, 2, :, cut]
            new_conv[layer, 2, :, cut] = fresh
            values = silu(acc)
            for at in range(0, block, LANES):
                lane0 = b * block + at
                head = lane0 // HEAD_DIM
                g = lane0 // span
                inner = jnp.sum(
                    in_vec[:, g * STATE_DIM : (g + 1) * STATE_DIM]
                    * out_vec[:, g * STATE_DIM : (g + 1) * STATE_DIM],
                    axis=1, keepdims=True,
                )
                v = values[:, at : at + LANES]
                drive = expand(step, head, rows_d) * v
                drive_pad[0:rows_d, lane0 : lane0 + LANES] = drive
                read_buf[:, lane0 : lane0 + LANES] = (
                    expand(decay, head, rows_d) * read_buf[:, lane0 : lane0 + LANES]
                    + drive * inner
                    + expand(skips, head, rows_d) * v
                )
        gain_row = out_gain[...].astype(F32)[layer : layer + 1]
        flown = []
        for b in range(blocks):
            c = blocks + b
            for copy in flights[1 + c]:
                copy.wait_recv()
            fresh = (total(send_proj.at[layer, c], recv_proj.at[layer, c]) * scale).astype(BF16)
            mixed = read_buf[:, b * block : (b + 1) * block] * silu(fresh.astype(F32))
            for at in range(0, block, span):
                cut = slice(b * block + at, b * block + at + span)
                part = mixed[:, at : at + span]
                mean = jnp.mean(part * part, axis=1, keepdims=True)
                held[layer, dp, :, cut] = (
                    part * lax.rsqrt(mean + EPS) * gain_row[:, cut]
                ).astype(BF16)
            copies = []
            for k in range(ndp - 1, 0, -1):
                cut = pl.ds(b * block, block)
                copy = remote(
                    held.at[layer, dp, :, cut], held.at[layer, dp, :, cut],
                    ssem_n.at[layer, b, k], rsem_n.at[layer, b, k], "dp", lax.rem(dp + k, ndp),
                )
                copy.start()
                copies.append(copy)
            pending.extend(copies)
            flown.append(copies)
        return flown

    def update_state(layer):
        for at in range(0, cols, LANES):
            drive_t[at : at + LANES, :] = jnp.transpose(drive_pad[:, at : at + LANES])

        def one_head(h, carry):
            decay_row = decay_t[pl.ds(h, 1), :]
            drive = drive_t[pl.ds(pl.multiple_of(h * HEAD_DIM, HEAD_DIM), HEAD_DIM), :]
            inp = ins_buf[h // group_heads]
            for r in range(rows_d):
                ssm_ref[layer, r, h] = ssm_ref[layer, r, h] * jnp.broadcast_to(
                    decay_row[:, r : r + 1], (HEAD_DIM, STATE_DIM)
                ) + jnp.broadcast_to(drive[:, r : r + 1], (HEAD_DIM, STATE_DIM)) * inp[r : r + 1, :]
            return carry

        lax.fori_loop(0, local_heads, one_head, 0)

    def gather_out(layer, flown):
        out_loads[layer].wait()
        acc = jnp.zeros((batch, width), F32)
        for b in range(blocks):
            for copy in flown[b]:
                copy.wait_recv()
            cut = slice(b * block, (b + 1) * block)
            for i in range(ndp):
                lhs_out[i * rows_d : (i + 1) * rows_d, cut] = held[layer, i, :, cut].astype(F32)
            acc = acc + jnp.dot(
                lhs_out[:, cut].astype(BF16), w_out[layer, cut, :], preferred_element_type=F32
            )
        return acc

    flights = project(0, lambda i: landed[i].astype(F32))
    for layer in range(LAYER_COUNT):
        state_loads.append(load(ssm_hbm.at[layer], ssm_ref.at[layer], ssm_sem.at[layer]))
        out_loads.append(load(w_out_hbm.at[layer], w_out.at[layer], weight_sem.at[layer, 4]))
        flown = head_step(layer, flights)
        last = layer == LAYER_COUNT - 1
        if not last:
            weights.append(load_weights(layer + 1))
        update_state(layer)
        acc = gather_out(layer, flown)
        if last:
            for i in range(ntp):
                send_out[i] = acc[i * rows_t : (i + 1) * rows_t].astype(BF16)
            finals = []
            for k in range(1, ntp):
                peer = lax.rem(tp + k, ntp)
                copy = remote(send_out.at[peer], recv_out.at[k], ssem_f.at[k], rsem_f.at[k], "tp", peer)
                copy.start()
                finals.append(copy)
            for copy in finals:
                copy.wait()
            total_out = send_out[tp].astype(F32)
            for k in range(1, ntp):
                total_out = total_out + recv_out[k].astype(F32)
            tok_ref[...] = (rows_buf[tp].astype(F32) + total_out).astype(BF16)
        else:
            part_out[layer] = acc.astype(BF16)
            parts = []
            for k in range(1, ntp):
                copy = remote(
                    part_out.at[layer], parts_in.at[layer, k], ssem_o.at[layer, k],
                    rsem_o.at[layer, k], "tp", lax.rem(tp + k, ntp),
                )
                copy.start()
                parts.append(copy)
            pending.extend(parts)
            for copy in parts:
                copy.wait_recv()
            acc = part_out[layer].astype(F32)
            for k in range(1, ntp):
                acc = acc + parts_in[layer, k].astype(F32)
            before = landed if layer == 0 else rows_buf

            def rows(i, before=before, acc=acc):
                part = (before[i].astype(F32) + acc[i * rows_t : (i + 1) * rows_t]).astype(BF16)
                rows_buf[i] = part
                return part.astype(F32)

            flights = project(layer + 1, rows)
    for copy in pending:
        copy.wait_send()


def write_kernel(tok, conv, vec, ssm, tok_out, conv_out, vec_out, ssm_out, sem, ssm_sem):
    copies = []
    layers, rows = ssm.shape[:2]
    for l in range(layers):
        for r in range(rows):
            copies.append(
                pltpu.make_async_copy(ssm.at[l, r], ssm_out.at[l, r], ssm_sem.at[l, r])
            )
    for i, (src, dst) in enumerate(((tok, tok_out), (conv, conv_out), (vec, vec_out))):
        copies.append(pltpu.make_async_copy(src, dst, sem.at[i]))
    for copy in copies:
        copy.start()
    for copy in copies:
        copy.wait()


VMEM = pl.BlockSpec(memory_space=pltpu.VMEM)
HBM = pl.BlockSpec(memory_space=pl.ANY)


def dma(*shape):
    return pltpu.SemaphoreType.DMA(shape)


def shards(
    ntp, ndp, tokens, w_in, w_vec, w_step, conv_weight, conv_vec, conv_state, vec_state,
    ssm_state, step_bias, decay_log, skip_gain, mix_gain, out_gain, w_out,
):
    rows_t, width = tokens.shape
    layers = w_in.shape[0]
    batch = rows_t * ntp
    rows_d = batch // ndp
    cols, vcols, heads = w_in.shape[3], w_vec.shape[3], w_step.shape[2]
    groups = vcols // STATE_DIM
    block = min(cols, 1024)
    chunks = 2 * cols // block
    small = 2 * vcols + LANES
    conv_rows = jnp.transpose(conv_state, (0, 2, 1, 3))
    vec_rows = jnp.transpose(vec_state, (0, 1, 3, 2, 4))
    scratch = [
        pltpu.VMEM(w_step.shape, BF16),
        pltpu.VMEM(w_in.shape, BF16),
        pltpu.VMEM(w_vec.shape, BF16),
        pltpu.VMEM(w_out.shape, BF16),
        pltpu.VMEM(mix_gain.shape, BF16),
        pltpu.VMEM(conv_weight.shape, BF16),
        pltpu.VMEM(conv_vec.shape, BF16),
        pltpu.VMEM(conv_rows.shape, BF16),
        pltpu.VMEM(vec_rows.shape, BF16),
        pltpu.VMEM(step_bias.shape, F32),
        pltpu.VMEM(decay_log.shape, F32),
        pltpu.VMEM(skip_gain.shape, F32),
        pltpu.VMEM(out_gain.shape, BF16),
        pltpu.VMEM((ntp, rows_t, width), BF16),
        pltpu.VMEM((batch, width), F32),
        pltpu.VMEM((layers, ndp, rows_d, small), BF16),
        pltpu.VMEM((layers, ndp, rows_d, small), BF16),
        pltpu.VMEM((layers, chunks, ndp, rows_d, block), BF16),
        pltpu.VMEM((layers, chunks, ndp, rows_d, block), BF16),
        pltpu.VMEM((groups, rows_d, STATE_DIM), F32),
        pltpu.VMEM((groups, rows_d, STATE_DIM), F32),
        pltpu.VMEM((rows_d, cols), F32),
        pltpu.VMEM((LANES, cols), F32),
        pltpu.VMEM((cols, LANES), F32),
        pltpu.VMEM((LANES, LANES), F32),
        pltpu.VMEM((LANES, LANES), F32),
        pltpu.VMEM((layers, ndp, rows_d, cols), BF16),
        pltpu.VMEM((batch, cols), F32),
        pltpu.VMEM((layers, batch, width), BF16),
        pltpu.VMEM((layers, ntp, batch, width), BF16),
        pltpu.VMEM((ntp, rows_t, width), BF16),
        pltpu.VMEM((ntp, rows_t, width), BF16),
        pltpu.VMEM((ntp, rows_t, width), BF16),
        dma(9), dma(layers, 5), dma(layers), dma(ntp), dma(ntp),
        dma(layers, ndp), dma(layers, ndp), dma(layers, chunks, ndp), dma(layers, chunks, ndp),
        dma(layers, chunks, ndp), dma(layers, chunks, ndp),
        dma(layers, ntp), dma(layers, ntp), dma(ntp), dma(ntp),
    ]
    results = pl.pallas_call(
        functools.partial(mixer_kernel, ntp, ndp),
        out_shape=(
            pltpu.VMEM(tokens.shape, BF16),
            pltpu.VMEM(conv_rows.shape, BF16),
            pltpu.VMEM(vec_rows.shape, BF16),
            pltpu.VMEM(ssm_state.shape, F32),
        ),
        in_specs=[VMEM] + [HBM] * 14,
        out_specs=(VMEM,) * 4,
        scratch_shapes=scratch,
        compiler_params=pltpu.CompilerParams(
            collective_id=0, has_side_effects=True, vmem_limit_bytes=44 << 20
        ),
    )(
        tokens, mix_gain, w_step, w_in, w_vec, w_out, conv_weight, conv_vec, conv_rows, vec_rows,
        ssm_state, step_bias, decay_log, skip_gain, out_gain,
    )
    new_tokens, new_conv, new_vec, new_ssm = pl.pallas_call(
        write_kernel,
        out_shape=tuple(jax.ShapeDtypeStruct(r.shape, r.dtype) for r in results),
        in_specs=[VMEM] * 4,
        out_specs=(HBM,) * 4,
        scratch_shapes=[dma(3), dma(layers, rows_d)],
        compiler_params=pltpu.CompilerParams(vmem_limit_bytes=8 << 20),
    )(*results)
    return (
        new_tokens,
        jnp.transpose(new_conv, (0, 2, 1, 3)),
        jnp.transpose(new_vec, (0, 1, 3, 2, 4)),
        new_ssm,
    )


def solution(mesh):
    placed = (
        P(("grp", "tp"), "dp"),
        P(None, None, "dp", "tp"),
        P(None, None, "dp", "tp"),
        P(None, "dp", None),
        P(None, None, "tp"),
        P(None, None, None, "tp"),
        P(None, ("grp", "dp"), None, "tp"),
        P(None, None, ("grp", "dp"), None, "tp"),
        P(None, ("grp", "dp"), "tp", None, None),
        P(None, "tp"),
        P(None, "tp"),
        P(None, "tp"),
        P(None, "dp"),
        P(None, "tp"),
        P(None, "tp", "dp"),
    )
    return jax.shard_map(
        functools.partial(shards, mesh.shape["tp"], mesh.shape["dp"]),
        mesh=mesh,
        in_specs=placed,
        out_specs=(
            P(("grp", "tp"), "dp"),
            P(None, ("grp", "dp"), None, "tp"),
            P(None, None, ("grp", "dp"), None, "tp"),
            P(None, ("grp", "dp"), "tp", None, None),
        ),
        check_vma=False,
    )
```

```python
import functools
import types

import jax
import jax.numpy as jnp
from jax import lax
from jax.experimental import pallas as pl
from jax.experimental.pallas import tpu as pltpu
from jax.sharding import PartitionSpec as P

MODEL_WIDTH = 4096
HEAD_DIM = 64
STATE_DIM = 128
LANES = 128
LAYER_COUNT = 2

EPS = 1e-06
F32 = jnp.float32
BF16 = jnp.bfloat16


def remote(src, dst, send_sem, recv_sem, axis, target):
    return pltpu.make_async_remote_copy(
        src_ref=src,
        dst_ref=dst,
        send_sem=send_sem,
        recv_sem=recv_sem,
        device_id={axis: target},
        device_id_type=pl.DeviceIdType.MESH,
    )


def greet(sizes):
    barrier = pltpu.get_barrier_semaphore()
    count = 0
    for axis, n in sizes:
        me = lax.axis_index(axis)
        for k in range(1, n):
            pl.semaphore_signal(
                barrier,
                inc=1,
                device_id={axis: lax.rem(me + k, n)},
                device_id_type=pl.DeviceIdType.MESH,
            )
            count += 1
    pl.semaphore_wait(barrier, count)


def silu(v):
    return v / (1.0 + jnp.exp(-v))


def softplus(v):
    return jnp.maximum(v, 0.0) + jnp.log1p(jnp.exp(-jnp.abs(v)))


def expand(per_head, at, rows):
    per = LANES // HEAD_DIM
    lane = lax.broadcasted_iota(jnp.int32, (rows, LANES), 1)
    out = jnp.broadcast_to(per_head[:, at : at + 1], (rows, LANES))
    for j in range(1, per):
        other = jnp.broadcast_to(per_head[:, at + j : at + j + 1], (rows, LANES))
        out = jnp.where(lane >= j * HEAD_DIM, other, out)
    return out


SEND_KINDS = ("x", "a", "b", "p", "n", "o")


def far_first(me, n):
    low = jnp.asarray(me < (n + 1) // 2, jnp.int32)
    out = []
    for j in range(n - 1):
        up = j + jnp.asarray(j >= me, jnp.int32)
        down = n - 1 - (j + jnp.asarray(j >= n - 1 - me, jnp.int32))
        out.append(low * down + (1 - low) * up)
    return out


def settle(ref, sem):
    pltpu.make_async_copy(ref, ref, sem).wait()


def mixer_kernel(ntp, ndp, names, *refs):
    s = types.SimpleNamespace(**dict(zip(names, refs)))
    outs = refs[len(names) - len(SCRATCH) - (ntp - 1) : len(names) - len(SCRATCH)]
    rows_t, width = s.x.shape
    batch = rows_t * ntp
    rows_d = batch // ndp
    cols = s.w_in.shape[3]
    vcols = s.w_vec.shape[3]
    heads = s.w_step.shape[2]
    local_heads = s.ssm.shape[2]
    groups = vcols // STATE_DIM
    span = cols // groups
    group_heads = local_heads // groups
    block = s.send_p.shape[4]
    blocks = cols // block
    tp = lax.axis_index("tp")
    dp = lax.axis_index("dp")
    far = far_first(dp, ndp)

    def load(src, dst, sem):
        copy = pltpu.make_async_copy(src, dst, sem)
        copy.start()
        return copy

    def load_weights(layer):
        vec = [
            load(s.w_vec_hbm.at[layer, role], s.w_vec.at[layer, role], s.weight_sem.at[layer, role])
            for role in (1, 0)
        ]
        step = load(s.w_step_hbm.at[layer], s.w_step.at[layer], s.weight_sem.at[layer, 2])
        return vec, step, [
            load(s.w_in_hbm.at[layer, role], s.w_in.at[layer, role], s.weight_sem.at[layer, 3 + role])
            for role in (1, 0)
        ]

    def load_rest(layer):
        return (
            load(s.ssm_hbm.at[layer], s.ssm.at[layer], s.weight_sem.at[layer, 5]),
            load(s.w_out_hbm.at[layer], s.w_out.at[layer], s.weight_sem.at[layer, 6]),
        )

    weights = [load_weights(0)]
    smalls = [
        load(getattr(s, name + "_hbm"), getattr(s, name), s.small_sem.at[i])
        for i, name in enumerate(SMALLS)
    ]
    greet((("tp", ntp), ("dp", ndp)))
    for k in range(1, ntp):
        remote(
            s.x, s.landed.at[tp], s.sent.at[0], s.got_x.at[0], "tp", lax.rem(tp + k, ntp)
        ).start()
    s.landed[tp] = s.x[...]
    s.drive_pad[...] = jnp.zeros_like(s.drive_pad)
    s.decay_pad[...] = jnp.zeros_like(s.decay_pad)
    s.outer[...] = jnp.zeros_like(s.outer)
    for copy in smalls:
        copy.wait()
    settle(s.landed.at[pl.ds(0, ntp - 1)], s.got_x.at[0])
    rest = [load_rest(0)]

    def project(layer, rows):
        scale_row = s.gain[...].astype(F32)[layer : layer + 1]
        squares = []
        for i in range(ntp):
            part = rows(i)
            squares.append(jnp.sum(part * part, axis=1, keepdims=True))
            s.lhs_buf[i * rows_t : (i + 1) * rows_t, :] = part * scale_row
        squares = jnp.concatenate(squares, axis=0)
        lhs = s.lhs_buf[...].astype(BF16)
        load_vec, load_step, load_in = weights[layer]

        def put(target, at, acc):
            for p in range(ndp):
                target[p, :, at : at + acc.shape[1]] = acc[p * rows_d : (p + 1) * rows_d].astype(
                    BF16
                )

        def deal(target, landing, kind, got):
            for peer in far:
                remote(
                    target.at[peer], landing.at[dp], s.sent.at[SEND_KINDS.index(kind)], got,
                    "dp", peer,
                ).start()

        load_vec[0].wait()
        put(s.send_a.at[layer], 0, jnp.dot(lhs, s.w_vec[layer, 1], preferred_element_type=F32))
        deal(s.send_a.at[layer], s.land_a.at[layer], "a", s.got_a.at[layer])
        load_step.wait()
        load_vec[1].wait()
        small = jnp.dot(lhs, s.w_step[layer], preferred_element_type=F32)
        small = pltpu.roll(small, lax.rem(heads - tp * local_heads, heads), 1)
        lane = lax.broadcasted_iota(jnp.int32, small.shape, 1)
        small = jnp.where(lane == local_heads, jnp.broadcast_to(squares, small.shape), small)
        put(s.send_b.at[layer], vcols, small)
        put(s.send_b.at[layer], 0, jnp.dot(lhs, s.w_vec[layer, 0], preferred_element_type=F32))
        deal(s.send_b.at[layer], s.land_b.at[layer], "b", s.got_b.at[layer])
        for j, role in enumerate((1, 0)):
            load_in[j].wait()
            for b in range(blocks):
                c = j * blocks + b
                acc = jnp.dot(
                    lhs, s.w_in[layer, role, :, b * block : (b + 1) * block],
                    preferred_element_type=F32,
                )
                put(s.send_p.at[layer, c], 0, acc)
                deal(s.send_p.at[layer, c], s.land_p.at[layer, c], "p", s.got_p.at[layer, c])

    def total(mine, others):
        acc = mine[dp].astype(F32)
        for k in range(1, ndp):
            acc = acc + others[lax.rem(dp + k, ndp)].astype(F32)
        return acc

    def arrived(landing, got):
        settle(landing.at[pl.ds(0, ndp - 1)], got)

    def head_step(layer):
        arrived(s.land_a.at[layer], s.got_a.at[layer])
        arrived(s.land_b.at[layer], s.got_b.at[layer])
        small = total(s.send_b.at[layer], s.land_b.at[layer])
        own_sq = small[:, vcols + local_heads : vcols + local_heads + 1]
        scale = lax.rsqrt(own_sq * (1.0 / MODEL_WIDTH) + EPS)
        taps_v = s.conv_v[layer].astype(F32)
        acts = []
        for role in range(2):
            raw = small[:, 0:vcols] if role == 0 else total(s.send_a.at[layer], s.land_a.at[layer])
            fresh = (raw * scale).astype(BF16)
            acc = fresh.astype(F32) * taps_v[role, 3:4]
            for i in range(3):
                acc = acc + s.vec_s[layer, role, i].astype(F32) * taps_v[role, i : i + 1]
            s.new_vec[layer, role, 0] = s.vec_s[layer, role, 1]
            s.new_vec[layer, role, 1] = s.vec_s[layer, role, 2]
            s.new_vec[layer, role, 2] = fresh
            acts.append(silu(acc))
        in_vec, out_vec = acts
        step = softplus(
            small[:, vcols : vcols + local_heads] * scale + s.bias[layer : layer + 1]
        )
        decay = jnp.exp(-step * jnp.exp(s.decay_log[layer : layer + 1]))
        s.decay_pad[0:rows_d, 0:local_heads] = decay
        s.decay_t[...] = jnp.transpose(s.decay_pad[...])
        rest[layer][0].wait()
        row = lax.broadcasted_iota(jnp.int32, (rows_d, STATE_DIM), 0)
        skips = jnp.broadcast_to(s.skip[layer : layer + 1], (rows_d, local_heads))
        inner = []
        for g in range(groups):
            in_g = in_vec[:, g * STATE_DIM : (g + 1) * STATE_DIM]
            out_g = out_vec[:, g * STATE_DIM : (g + 1) * STATE_DIM]
            inner.append(jnp.sum(in_g * out_g, axis=1, keepdims=True))
            acc = jnp.zeros((rows_d, span), F32)
            for r in range(rows_d):
                mine = jnp.where(row == r, out_g, 0.0)
                state = s.ssm[layer, r, g * group_heads : (g + 1) * group_heads]
                acc = acc + lax.dot_general(
                    mine, state.reshape(span, STATE_DIM), (((1,), (1,)), ((), ())),
                    preferred_element_type=F32,
                )
            s.read[:, g * span : (g + 1) * span] = acc
            high = in_g.astype(BF16).astype(F32)
            for r in range(rows_d):
                at = (r % 2) * STATE_DIM
                lanes = slice(at, at + STATE_DIM)
                mine = jnp.where(row == r, high, 0.0)
                s.outer[g, r // 2, 0:rows_d, lanes] = mine
                s.outer[g, r // 2, rows_d : 2 * rows_d, lanes] = mine
                s.outer[g, r // 2, 2 * rows_d : 3 * rows_d, lanes] = jnp.where(
                    row == r, in_g - high, 0.0
                )
        taps = s.conv_w[layer].astype(F32)
        for b in range(blocks):
            arrived(s.land_p.at[layer, b], s.got_p.at[layer, b])
            cut = slice(b * block, (b + 1) * block)
            fresh = (total(s.send_p.at[layer, b], s.land_p.at[layer, b]) * scale).astype(BF16)
            acc = fresh.astype(F32) * taps[3:4, cut]
            for i in range(3):
                acc = acc + s.conv_s[layer, i, :, cut].astype(F32) * taps[i : i + 1, cut]
            s.new_conv[layer, 0, :, cut] = s.conv_s[layer, 1, :, cut]
            s.new_conv[layer, 1, :, cut] = s.conv_s[layer, 2, :, cut]
            s.new_conv[layer, 2, :, cut] = fresh
            values = silu(acc)
            for at in range(0, block, LANES):
                lane0 = b * block + at
                head = lane0 // HEAD_DIM
                v = values[:, at : at + LANES]
                drive = expand(step, head, rows_d) * v
                lanes = slice(lane0, lane0 + LANES)
                high = drive.astype(BF16).astype(F32)
                s.drive_pad[0:rows_d, lanes] = high
                s.drive_pad[rows_d : 2 * rows_d, lanes] = drive - high
                s.drive_pad[2 * rows_d : 3 * rows_d, lanes] = high
                s.read[:, lanes] = (
                    expand(decay, head, rows_d) * s.read[:, lanes]
                    + drive * inner[lane0 // span]
                    + expand(skips, head, rows_d) * v
                )
        for at in range(0, cols, LANES):
            s.drive_t[at : at + LANES, :] = jnp.transpose(s.drive_pad[:, at : at + LANES])
        gain_row = s.out_gain[...].astype(F32)[layer : layer + 1]
        for b in range(blocks):
            c = blocks + b
            arrived(s.land_p.at[layer, c], s.got_p.at[layer, c])
            fresh = (total(s.send_p.at[layer, c], s.land_p.at[layer, c]) * scale).astype(BF16)
            mixed = s.read[:, b * block : (b + 1) * block] * silu(fresh.astype(F32))
            for at in range(0, block, span):
                cut = slice(b * block + at, b * block + at + span)
                part = mixed[:, at : at + span]
                mean = jnp.mean(part * part, axis=1, keepdims=True)
                s.held[layer, dp, :, cut] = (
                    part * lax.rsqrt(mean + EPS) * gain_row[:, cut]
                ).astype(BF16)
            mine = s.held.at[layer, dp, :, pl.ds(b * block, block)]
            for peer in far:
                remote(
                    mine, mine, s.sent.at[SEND_KINDS.index("n")], s.got_n.at[layer, b], "dp", peer
                ).start()

    def update_state(layer):
        some = min(4, group_heads)

        def some_heads(q, carry):
            first = q * some
            lhs = s.drive_t[pl.ds(pl.multiple_of(first * HEAD_DIM, HEAD_DIM), some * HEAD_DIM), :]
            for pair in range(rows_d // 2):
                added = jnp.dot(
                    lhs, s.outer[first // group_heads, pair], preferred_element_type=F32
                )
                for r in (2 * pair, 2 * pair + 1):
                    at = (r % 2) * STATE_DIM
                    for j in range(some):
                        decay = s.decay_t[pl.ds(first + j, 1), :][:, r : r + 1]
                        s.ssm[layer, r, first + j] = (
                            s.ssm[layer, r, first + j]
                            * jnp.broadcast_to(decay, (HEAD_DIM, STATE_DIM))
                            + added[j * HEAD_DIM : (j + 1) * HEAD_DIM, at : at + STATE_DIM]
                        )
            return carry

        lax.fori_loop(0, local_heads // some, some_heads, 0)

    def gather_out(layer):
        rest[layer][1].wait()
        acc = jnp.zeros((batch, width), F32)
        for b in range(blocks):
            cut = slice(b * block, (b + 1) * block)
            settle(s.held.at[layer, pl.ds(0, ndp - 1), :, pl.ds(b * block, block)], s.got_n.at[layer, b])
            for i in range(ndp):
                s.lhs_out[i * rows_d : (i + 1) * rows_d, cut] = s.held[layer, i, :, cut].astype(F32)
            acc = acc + jnp.dot(
                s.lhs_out[:, cut].astype(BF16), s.w_out[layer, cut, :], preferred_element_type=F32
            )
        return acc

    project(0, lambda i: s.landed[i].astype(F32))
    for layer in range(LAYER_COUNT):
        last = layer == LAYER_COUNT - 1
        if not last:
            weights.append(load_weights(layer + 1))
            rest.append(load_rest(layer + 1))
        head_step(layer)
        update_state(layer)
        acc = gather_out(layer)
        if last:
            for i in range(ntp):
                s.sums[i] = acc[i * rows_t : (i + 1) * rows_t]
            s.base[...] = s.rows[tp].astype(F32) + s.sums[tp]
            for k in range(1, ntp):
                outs[k - 1][...] = s.sums[lax.rem(tp + k, ntp)].astype(BF16)
        else:
            s.part_out[layer] = acc.astype(BF16)
            for k in range(1, ntp):
                remote(
                    s.part_out.at[layer], s.parts_in.at[layer, tp],
                    s.sent.at[SEND_KINDS.index("o")], s.got_o.at[layer],
                    "tp", lax.rem(tp + k, ntp),
                ).start()
            settle(s.parts_in.at[layer, pl.ds(0, ntp - 1)], s.got_o.at[layer])
            s.parts_in[layer, tp] = s.part_out[layer]
            acc = s.parts_in[layer, 0].astype(F32)
            for i in range(1, ntp):
                acc = acc + s.parts_in[layer, i].astype(F32)
            before = s.landed if layer == 0 else s.rows

            def rows(i, before=before, acc=acc):
                part = (before[i].astype(F32) + acc[i * rows_t : (i + 1) * rows_t]).astype(BF16)
                s.rows[i] = part
                return part.astype(F32)

            project(layer + 1, rows)
    settle(s.landed.at[pl.ds(0, ntp - 1)], s.sent.at[0])
    settle(s.send_a.at[:, pl.ds(0, ndp - 1)], s.sent.at[1])
    settle(s.send_b.at[:, pl.ds(0, ndp - 1)], s.sent.at[2])
    settle(s.send_p.at[:, :, pl.ds(0, ndp - 1)], s.sent.at[3])
    settle(s.held.at[:, pl.ds(0, ndp - 1)], s.sent.at[4])
    settle(s.parts_in.at[:, pl.ds(0, ntp - 1)], s.sent.at[5])


def write_kernel(conv, vec, ssm, conv_out, vec_out, ssm_out, sem, ssm_sem):
    layers, rows = ssm.shape[:2]
    for l in range(layers):
        for r in range(rows):
            pltpu.make_async_copy(ssm.at[l, r], ssm_out.at[l, r], ssm_sem).start()
    others = []
    for i, (src, dst) in enumerate(((conv, conv_out), (vec, vec_out))):
        others.append(pltpu.make_async_copy(src, dst, sem.at[i]))
        others[-1].start()
    for copy in others:
        copy.wait()
    pltpu.make_async_copy(ssm, ssm_out, ssm_sem).wait()


VMEM = pl.BlockSpec(memory_space=pltpu.VMEM)
HBM = pl.BlockSpec(memory_space=pl.ANY)


def dma(*shape):
    return pltpu.SemaphoreType.DMA(shape)


SMALLS = (
    "gain", "conv_w", "conv_v", "conv_s", "vec_s", "bias", "decay_log", "skip", "out_gain"
)
INPUTS = ("x", "w_step_hbm", "w_in_hbm", "w_vec_hbm", "w_out_hbm", "ssm_hbm") + tuple(
    name + "_hbm" for name in SMALLS
)
SCRATCH = (
    "w_step", "w_in", "w_vec", "w_out",
) + SMALLS + (
    "landed", "lhs_buf", "send_a", "land_a", "send_b", "land_b", "send_p", "land_p",
    "read", "drive_pad", "drive_t", "outer", "decay_pad", "decay_t",
    "held", "lhs_out", "part_out", "parts_in", "rows", "sums",
    "small_sem", "weight_sem", "sent", "got_x", "got_a", "got_b", "got_p", "got_n", "got_o",
)


def shards(
    ntp, ndp, tokens, w_in, w_vec, w_step, conv_weight, conv_vec, conv_state, vec_state,
    ssm_state, step_bias, decay_log, skip_gain, mix_gain, out_gain, w_out,
):
    rows_t, width = tokens.shape
    layers = w_in.shape[0]
    batch = rows_t * ntp
    rows_d = batch // ndp
    cols, vcols = w_in.shape[3], w_vec.shape[3]
    groups = vcols // STATE_DIM
    block = min(cols, 1024)
    chunks = 2 * cols // block
    conv_rows = jnp.transpose(conv_state, (0, 2, 1, 3))
    vec_rows = jnp.transpose(vec_state, (0, 1, 3, 2, 4))
    smalls = (
        mix_gain, conv_weight, conv_vec, conv_rows, vec_rows, step_bias, decay_log, skip_gain,
        out_gain,
    )
    scratch = [pltpu.VMEM(a.shape, a.dtype) for a in (w_step, w_in, w_vec, w_out) + smalls] + [
        pltpu.VMEM((ntp, rows_t, width), BF16),
        pltpu.VMEM((batch, width), F32),
        pltpu.VMEM((layers, ndp, rows_d, vcols), BF16),
        pltpu.VMEM((layers, ndp, rows_d, vcols), BF16),
        pltpu.VMEM((layers, ndp, rows_d, vcols + LANES), BF16),
        pltpu.VMEM((layers, ndp, rows_d, vcols + LANES), BF16),
        pltpu.VMEM((layers, chunks, ndp, rows_d, block), BF16),
        pltpu.VMEM((layers, chunks, ndp, rows_d, block), BF16),
        pltpu.VMEM((rows_d, cols), F32),
        pltpu.VMEM((LANES, cols), F32),
        pltpu.VMEM((cols, LANES), F32),
        pltpu.VMEM((groups, rows_d // 2, LANES, 2 * STATE_DIM), F32),
        pltpu.VMEM((LANES, LANES), F32),
        pltpu.VMEM((LANES, LANES), F32),
        pltpu.VMEM((layers, ndp, rows_d, cols), BF16),
        pltpu.VMEM((batch, cols), F32),
        pltpu.VMEM((layers - 1, batch, width), BF16),
        pltpu.VMEM((layers - 1, ntp, batch, width), BF16),
        pltpu.VMEM((ntp, rows_t, width), BF16),
        pltpu.VMEM((ntp, rows_t, width), F32),
        dma(len(SMALLS)), dma(layers, 7), dma(6), dma(1), dma(layers), dma(layers),
        dma(layers, chunks), dma(layers, chunks // 2), dma(layers - 1),
    ]
    out_shape = (
        pltpu.VMEM(tokens.shape, F32),
        pltpu.VMEM(conv_rows.shape, BF16),
        pltpu.VMEM(vec_rows.shape, BF16),
        pltpu.VMEM(ssm_state.shape, F32),
    ) + tuple(pltpu.VMEM(tokens.shape, BF16) for _ in range(ntp - 1))
    names = (
        INPUTS + ("base", "new_conv", "new_vec", "ssm")
        + tuple(f"out{k}" for k in range(1, ntp)) + SCRATCH
    )
    base, new_conv, new_vec, new_ssm, *parts = pl.pallas_call(
        functools.partial(mixer_kernel, ntp, ndp, names),
        out_shape=out_shape,
        in_specs=[VMEM] + [HBM] * (len(INPUTS) - 1),
        out_specs=(VMEM,) * len(out_shape),
        scratch_shapes=scratch,
        compiler_params=pltpu.CompilerParams(
            collective_id=0, has_side_effects=True, vmem_limit_bytes=44 << 20
        ),
    )(tokens, w_step, w_in, w_vec, w_out, ssm_state, *smalls)
    parts = [
        lax.ppermute(part, "tp", [(i, (i + k) % ntp) for i in range(ntp)])
        for k, part in enumerate(parts, 1)
    ]
    results = (new_conv, new_vec, new_ssm)
    new_conv, new_vec, new_ssm = pl.pallas_call(
        write_kernel,
        out_shape=tuple(jax.ShapeDtypeStruct(r.shape, r.dtype) for r in results),
        in_specs=[VMEM] * 3,
        out_specs=(HBM,) * 3,
        scratch_shapes=[dma(2), pltpu.SemaphoreType.DMA],
        compiler_params=pltpu.CompilerParams(vmem_limit_bytes=8 << 20),
        cost_estimate=pl.CostEstimate(
            flops=40_000_000, bytes_accessed=2 * new_ssm.size * 4, transcendentals=0
        ),
    )(*results)
    total = base
    for part in parts:
        total = total + part.astype(F32)
    return (
        total.astype(BF16),
        jnp.transpose(new_conv, (0, 2, 1, 3)),
        jnp.transpose(new_vec, (0, 1, 3, 2, 4)),
        new_ssm,
    )


def solution(mesh):
    placed = (
        P(("grp", "tp"), "dp"),
        P(None, None, "dp", "tp"),
        P(None, None, "dp", "tp"),
        P(None, "dp", None),
        P(None, None, "tp"),
        P(None, None, None, "tp"),
        P(None, ("grp", "dp"), None, "tp"),
        P(None, None, ("grp", "dp"), None, "tp"),
        P(None, ("grp", "dp"), "tp", None, None),
        P(None, "tp"),
        P(None, "tp"),
        P(None, "tp"),
        P(None, "dp"),
        P(None, "tp"),
        P(None, "tp", "dp"),
    )
    return jax.shard_map(
        functools.partial(shards, mesh.shape["tp"], mesh.shape["dp"]),
        mesh=mesh,
        in_specs=placed,
        out_specs=(
            P(("grp", "tp"), "dp"),
            P(None, ("grp", "dp"), None, "tp"),
            P(None, None, ("grp", "dp"), None, "tp"),
            P(None, ("grp", "dp"), "tp", None, None),
        ),
        check_vma=False,
    )
```

```python
import functools
import types

import jax
import jax.numpy as jnp
from jax import lax
from jax.experimental import pallas as pl
from jax.experimental.pallas import tpu as pltpu
from jax.sharding import PartitionSpec as P

MODEL_WIDTH = 4096
HEAD_DIM = 64
STATE_DIM = 128
LANES = 128
LAYER_COUNT = 2

EPS = 1e-06
F32 = jnp.float32
BF16 = jnp.bfloat16


def remote(src, dst, send_sem, recv_sem, axis, target):
    return pltpu.make_async_remote_copy(
        src_ref=src,
        dst_ref=dst,
        send_sem=send_sem,
        recv_sem=recv_sem,
        device_id={axis: target},
        device_id_type=pl.DeviceIdType.MESH,
    )


def greet(sizes):
    barrier = pltpu.get_barrier_semaphore()
    count = 0
    for axis, n in sizes:
        me = lax.axis_index(axis)
        for k in range(1, n):
            pl.semaphore_signal(
                barrier,
                inc=1,
                device_id={axis: lax.rem(me + k, n)},
                device_id_type=pl.DeviceIdType.MESH,
            )
            count += 1
    pl.semaphore_wait(barrier, count)


def silu(v):
    return v / (1.0 + jnp.exp(-v))


def softplus(v):
    return jnp.maximum(v, 0.0) + jnp.log1p(jnp.exp(-jnp.abs(v)))


def expand(per_head, at, rows):
    per = LANES // HEAD_DIM
    lane = lax.broadcasted_iota(jnp.int32, (rows, LANES), 1)
    out = jnp.broadcast_to(per_head[:, at : at + 1], (rows, LANES))
    for j in range(1, per):
        other = jnp.broadcast_to(per_head[:, at + j : at + j + 1], (rows, LANES))
        out = jnp.where(lane >= j * HEAD_DIM, other, out)
    return out


SEND_KINDS = ("x", "a", "b", "p", "n", "o", "f")


def far_first(me, n):
    low = jnp.asarray(me < (n + 1) // 2, jnp.int32)
    out = []
    for j in range(n - 1):
        up = j + jnp.asarray(j >= me, jnp.int32)
        down = n - 1 - (j + jnp.asarray(j >= n - 1 - me, jnp.int32))
        out.append(low * down + (1 - low) * up)
    return out


def settle(ref, sem):
    pltpu.make_async_copy(ref, ref, sem).wait()


def mixer_kernel(ntp, ndp, names, *refs):
    s = types.SimpleNamespace(**dict(zip(names, refs)))
    rows_t, width = s.tokens.shape
    batch = rows_t * ntp
    rows_d = batch // ndp
    cols = s.w_in.shape[3]
    vcols = s.w_vec.shape[3]
    heads = s.w_step.shape[2]
    local_heads = s.ssm.shape[2]
    groups = vcols // STATE_DIM
    span = cols // groups
    group_heads = local_heads // groups
    block = s.send_p.shape[4]
    blocks = cols // block
    tp = lax.axis_index("tp")
    dp = lax.axis_index("dp")
    far = far_first(dp, ndp)
    relay = ndp == 4
    at_end = jnp.logical_or(dp == 0, dp == ndp - 1)
    inside = jnp.logical_not(at_end)
    across = ndp - 1 - dp

    def load(src, dst, sem):
        copy = pltpu.make_async_copy(src, dst, sem)
        copy.start()
        return copy

    def load_weights(layer):
        vec = [
            load(s.w_vec_hbm.at[layer, role], s.w_vec.at[layer, role], s.weight_sem.at[layer, role])
            for role in (1, 0)
        ]
        step = load(s.w_step_hbm.at[layer], s.w_step.at[layer], s.weight_sem.at[layer, 2])
        return vec, step, [
            load(s.w_in_hbm.at[layer, role], s.w_in.at[layer, role], s.weight_sem.at[layer, 3 + role])
            for role in (1, 0)
        ]

    def load_rest(layer):
        return (
            load(s.ssm_hbm.at[layer], s.ssm.at[layer], s.weight_sem.at[layer, 5]),
            load(s.w_out_hbm.at[layer], s.w_out.at[layer], s.weight_sem.at[layer, 6]),
        )

    own = load(s.x_hbm, s.landed.at[tp], s.own_sem.at[0])
    weights = [load_weights(0)]
    smalls = [
        load(getattr(s, name + "_hbm"), getattr(s, name), s.small_sem.at[i])
        for i, name in enumerate(SMALLS)
    ]
    greet((("tp", ntp), ("dp", ndp)))
    own.wait()
    for k in range(1, ntp):
        remote(
            s.landed.at[tp], s.landed.at[tp], s.sent.at[0], s.got_x.at[0],
            "tp", lax.rem(tp + k, ntp),
        ).start()
    s.drive_pad[...] = jnp.zeros_like(s.drive_pad)
    s.decay_pad[...] = jnp.zeros_like(s.decay_pad)
    s.outer[...] = jnp.zeros_like(s.outer)
    if relay:
        @pl.when(at_end)
        def _():
            for layer in range(LAYER_COUNT):
                for c in range(2 * blocks - 1):
                    s.land_p[layer, c, across] = jnp.zeros((rows_d, block), BF16)

    for copy in smalls:
        copy.wait()
    settle(s.landed.at[pl.ds(0, ntp - 1)], s.got_x.at[0])
    rest = [load_rest(0)]

    def send_part(layer, c, peer):
        remote(
            s.send_p.at[layer, c, peer], s.land_p.at[layer, c, dp],
            s.sent.at[SEND_KINDS.index("p")], s.got_p.at[layer, c], "dp", peer,
        ).start()

    def deal_relayed(layer, c):
        @pl.when(at_end)
        def _():
            near = jnp.where(dp == 0, 1, ndp - 2)
            remote(
                s.send_p.at[layer, c, across], s.land_r.at[layer, c],
                s.sent.at[SEND_KINDS.index("p")], s.got_r.at[layer, c], "dp", near,
            ).start()
            send_part(layer, c, ndp - 1 - near)
            send_part(layer, c, near)

        @pl.when(inside)
        def _():
            send_part(layer, c, across)
            send_part(layer, c, (dp - 1) * 3)

    def project(layer, rows):
        scale_row = s.gain[...].astype(F32)[layer : layer + 1]
        squares = []
        for i in range(ntp):
            part = rows(i)
            squares.append(jnp.sum(part * part, axis=1, keepdims=True))
            s.lhs_buf[i * rows_t : (i + 1) * rows_t, :] = part * scale_row
        squares = jnp.concatenate(squares, axis=0)
        lhs = s.lhs_buf[...].astype(BF16)
        load_vec, load_step, load_in = weights[layer]

        def put(target, at, acc):
            for p in range(ndp):
                target[p, :, at : at + acc.shape[1]] = acc[p * rows_d : (p + 1) * rows_d].astype(
                    BF16
                )

        def deal(target, landing, kind, got):
            for peer in far:
                remote(
                    target.at[peer], landing.at[dp], s.sent.at[SEND_KINDS.index(kind)], got,
                    "dp", peer,
                ).start()

        load_vec[0].wait()
        put(s.send_a.at[layer], 0, jnp.dot(lhs, s.w_vec[layer, 1], preferred_element_type=F32))
        deal(s.send_a.at[layer], s.land_a.at[layer], "a", s.got_a.at[layer])
        load_step.wait()
        load_vec[1].wait()
        small = jnp.dot(lhs, s.w_step[layer], preferred_element_type=F32)
        small = pltpu.roll(small, lax.rem(heads - tp * local_heads, heads), 1)
        lane = lax.broadcasted_iota(jnp.int32, small.shape, 1)
        small = jnp.where(lane == local_heads, jnp.broadcast_to(squares, small.shape), small)
        put(s.send_b.at[layer], vcols, small)
        put(s.send_b.at[layer], 0, jnp.dot(lhs, s.w_vec[layer, 0], preferred_element_type=F32))
        deal(s.send_b.at[layer], s.land_b.at[layer], "b", s.got_b.at[layer])
        for j, role in enumerate((1, 0)):
            load_in[j].wait()
            for b in range(blocks):
                c = j * blocks + b
                acc = jnp.dot(
                    lhs, s.w_in[layer, role, :, b * block : (b + 1) * block],
                    preferred_element_type=F32,
                )
                put(s.send_p.at[layer, c], 0, acc)
                if relay and c < 2 * blocks - 1:
                    deal_relayed(layer, c)
                else:
                    deal(s.send_p.at[layer, c], s.land_p.at[layer, c], "p", s.got_p.at[layer, c])
        if relay:
            @pl.when(inside)
            def _():
                end = (dp - 1) * 3
                other = 3 - end
                for c in range(2 * blocks - 1):
                    settle(s.land_r.at[layer, c], s.got_r.at[layer, c])
                    s.send_p[layer, c, other] = (
                        s.send_p[layer, c, other].astype(F32) + s.land_r[layer, c].astype(F32)
                    ).astype(BF16)
                    send_part(layer, c, other)

    def total(mine, others):
        acc = mine[dp].astype(F32)
        for k in range(1, ndp):
            acc = acc + others[lax.rem(dp + k, ndp)].astype(F32)
        return acc

    def arrived(landing, got):
        settle(landing.at[pl.ds(0, ndp - 1)], got)

    def arrived_part(layer, c):
        if relay and c < 2 * blocks - 1:
            @pl.when(at_end)
            def _():
                settle(s.land_p.at[layer, c, pl.ds(0, ndp - 2)], s.got_p.at[layer, c])

            @pl.when(inside)
            def _():
                settle(s.land_p.at[layer, c, pl.ds(0, ndp - 1)], s.got_p.at[layer, c])
        else:
            arrived(s.land_p.at[layer, c], s.got_p.at[layer, c])

    def head_step(layer):
        arrived(s.land_a.at[layer], s.got_a.at[layer])
        arrived(s.land_b.at[layer], s.got_b.at[layer])
        small = total(s.send_b.at[layer], s.land_b.at[layer])
        own_sq = small[:, vcols + local_heads : vcols + local_heads + 1]
        scale = lax.rsqrt(own_sq * (1.0 / MODEL_WIDTH) + EPS)
        taps_v = s.conv_v[layer].astype(F32)
        acts = []
        for role in range(2):
            raw = small[:, 0:vcols] if role == 0 else total(s.send_a.at[layer], s.land_a.at[layer])
            fresh = (raw * scale).astype(BF16)
            acc = fresh.astype(F32) * taps_v[role, 3:4]
            for i in range(3):
                acc = acc + s.vec_s[layer, role, i].astype(F32) * taps_v[role, i : i + 1]
            s.new_vec[layer, role, 0] = s.vec_s[layer, role, 1]
            s.new_vec[layer, role, 1] = s.vec_s[layer, role, 2]
            s.new_vec[layer, role, 2] = fresh
            acts.append(silu(acc))
        in_vec, out_vec = acts
        step = softplus(
            small[:, vcols : vcols + local_heads] * scale + s.bias[layer : layer + 1]
        )
        decay = jnp.exp(-step * jnp.exp(s.decay_log[layer : layer + 1]))
        s.decay_pad[0:rows_d, 0:local_heads] = decay
        s.decay_t[...] = jnp.transpose(s.decay_pad[...])
        rest[layer][0].wait()
        row = lax.broadcasted_iota(jnp.int32, (rows_d, STATE_DIM), 0)
        skips = jnp.broadcast_to(s.skip[layer : layer + 1], (rows_d, local_heads))
        inner = []
        for g in range(groups):
            in_g = in_vec[:, g * STATE_DIM : (g + 1) * STATE_DIM]
            out_g = out_vec[:, g * STATE_DIM : (g + 1) * STATE_DIM]
            inner.append(jnp.sum(in_g * out_g, axis=1, keepdims=True))
            acc = jnp.zeros((rows_d, span), F32)
            for r in range(rows_d):
                mine = jnp.where(row == r, out_g, 0.0)
                state = s.ssm[layer, r, g * group_heads : (g + 1) * group_heads]
                acc = acc + lax.dot_general(
                    mine, state.reshape(span, STATE_DIM), (((1,), (1,)), ((), ())),
                    preferred_element_type=F32,
                )
            s.read[:, g * span : (g + 1) * span] = acc
            high = in_g.astype(BF16).astype(F32)
            for r in range(rows_d):
                at = (r % 2) * STATE_DIM
                lanes = slice(at, at + STATE_DIM)
                mine = jnp.where(row == r, high, 0.0)
                s.outer[g, r // 2, 0:rows_d, lanes] = mine
                s.outer[g, r // 2, rows_d : 2 * rows_d, lanes] = mine
                s.outer[g, r // 2, 2 * rows_d : 3 * rows_d, lanes] = jnp.where(
                    row == r, in_g - high, 0.0
                )
        taps = s.conv_w[layer].astype(F32)
        for b in range(blocks):
            arrived_part(layer, b)
            cut = slice(b * block, (b + 1) * block)
            fresh = (total(s.send_p.at[layer, b], s.land_p.at[layer, b]) * scale).astype(BF16)
            acc = fresh.astype(F32) * taps[3:4, cut]
            for i in range(3):
                acc = acc + s.conv_s[layer, i, :, cut].astype(F32) * taps[i : i + 1, cut]
            s.new_conv[layer, 0, :, cut] = s.conv_s[layer, 1, :, cut]
            s.new_conv[layer, 1, :, cut] = s.conv_s[layer, 2, :, cut]
            s.new_conv[layer, 2, :, cut] = fresh
            values = silu(acc)
            for at in range(0, block, LANES):
                lane0 = b * block + at
                head = lane0 // HEAD_DIM
                v = values[:, at : at + LANES]
                drive = expand(step, head, rows_d) * v
                lanes = slice(lane0, lane0 + LANES)
                high = drive.astype(BF16).astype(F32)
                s.drive_pad[0:rows_d, lanes] = high
                s.drive_pad[rows_d : 2 * rows_d, lanes] = drive - high
                s.drive_pad[2 * rows_d : 3 * rows_d, lanes] = high
                s.read[:, lanes] = (
                    expand(decay, head, rows_d) * s.read[:, lanes]
                    + drive * inner[lane0 // span]
                    + expand(skips, head, rows_d) * v
                )
        for at in range(0, cols, LANES):
            s.drive_t[at : at + LANES, :] = jnp.transpose(s.drive_pad[:, at : at + LANES])
        gain_row = s.out_gain[...].astype(F32)[layer : layer + 1]
        for b in range(blocks):
            c = blocks + b
            arrived_part(layer, c)
            fresh = (total(s.send_p.at[layer, c], s.land_p.at[layer, c]) * scale).astype(BF16)
            mixed = s.read[:, b * block : (b + 1) * block] * silu(fresh.astype(F32))
            for at in range(0, block, span):
                cut = slice(b * block + at, b * block + at + span)
                part = mixed[:, at : at + span]
                mean = jnp.mean(part * part, axis=1, keepdims=True)
                s.held[layer, dp, :, cut] = (
                    part * lax.rsqrt(mean + EPS) * gain_row[:, cut]
                ).astype(BF16)
            mine = s.held.at[layer, dp, :, pl.ds(b * block, block)]
            for peer in far:
                remote(
                    mine, mine, s.sent.at[SEND_KINDS.index("n")], s.got_n.at[layer, b], "dp", peer
                ).start()

    def update_state(layer):
        some = min(4, group_heads)

        def some_heads(q, carry):
            first = q * some
            lhs = s.drive_t[pl.ds(pl.multiple_of(first * HEAD_DIM, HEAD_DIM), some * HEAD_DIM), :]
            for pair in range(rows_d // 2):
                added = jnp.dot(
                    lhs, s.outer[first // group_heads, pair], preferred_element_type=F32
                )
                for r in (2 * pair, 2 * pair + 1):
                    at = (r % 2) * STATE_DIM
                    for j in range(some):
                        decay = s.decay_t[pl.ds(first + j, 1), :][:, r : r + 1]
                        s.ssm[layer, r, first + j] = (
                            s.ssm[layer, r, first + j]
                            * jnp.broadcast_to(decay, (HEAD_DIM, STATE_DIM))
                            + added[j * HEAD_DIM : (j + 1) * HEAD_DIM, at : at + STATE_DIM]
                        )
            return carry

        lax.fori_loop(0, local_heads // some, some_heads, 0)

    def gather_out(layer, emit):
        rest[layer][1].wait()
        half = width // 2
        accs = [jnp.zeros((batch, half), F32)] * 2
        for b in range(blocks):
            cut = slice(b * block, (b + 1) * block)
            settle(s.held.at[layer, pl.ds(0, ndp - 1), :, pl.ds(b * block, block)], s.got_n.at[layer, b])
            for i in range(ndp):
                s.lhs_out[i * rows_d : (i + 1) * rows_d, cut] = s.held[layer, i, :, cut].astype(F32)
            lhs = s.lhs_out[:, cut].astype(BF16)
            for h in range(2):
                accs[h] = accs[h] + jnp.dot(
                    lhs, s.w_out[layer, cut, h * half : (h + 1) * half], preferred_element_type=F32
                )
                if b == blocks - 1:
                    emit(h, accs[h])

    project(0, lambda i: s.landed[i].astype(F32))
    for layer in range(LAYER_COUNT):
        last = layer == LAYER_COUNT - 1
        if not last:
            weights.append(load_weights(layer + 1))
            rest.append(load_rest(layer + 1))
        head_step(layer)
        update_state(layer)
        half = width // 2

        def emit(h, acc, layer=layer, last=last):
            kind = s.sent.at[SEND_KINDS.index("f" if last else "o")]
            got = (s.got_f if last else s.got_o).at[0 if last else layer, h]
            if last:
                for i in range(ntp):
                    s.send_f[h, i] = acc[i * rows_t : (i + 1) * rows_t].astype(BF16)
            else:
                s.parts[layer, h, tp] = acc.astype(BF16)
            for k in range(1, ntp):
                peer = lax.rem(tp + k, ntp)
                src = s.send_f.at[h, peer] if last else s.parts.at[layer, h, tp]
                dst = s.land_f.at[h, tp] if last else src
                remote(src, dst, kind, got, "tp", peer).start()

        gather_out(layer, emit)
        if last:
            for h in range(2):
                cut = slice(h * half, (h + 1) * half)
                settle(s.land_f.at[h, pl.ds(0, ntp - 1)], s.got_f.at[0, h])
                s.land_f[h, tp] = s.send_f[h, tp]
                acc = s.rows[tp, :, cut].astype(F32)
                for i in range(ntp):
                    acc = acc + s.land_f[h, i].astype(F32)
                s.tokens[:, cut] = acc.astype(BF16)
        else:
            accs = []
            for h in range(2):
                settle(s.parts.at[layer, h, pl.ds(0, ntp - 1)], s.got_o.at[layer, h])
                acc = s.parts[layer, h, 0].astype(F32)
                for i in range(1, ntp):
                    acc = acc + s.parts[layer, h, i].astype(F32)
                accs.append(acc)
            acc = jnp.concatenate(accs, axis=1)
            before = s.landed if layer == 0 else s.rows

            def rows(i, before=before, acc=acc):
                part = (before[i].astype(F32) + acc[i * rows_t : (i + 1) * rows_t]).astype(BF16)
                s.rows[i] = part
                return part.astype(F32)

            project(layer + 1, rows)
    settle(s.landed.at[pl.ds(0, ntp - 1)], s.sent.at[0])
    settle(s.send_a.at[:, pl.ds(0, ndp - 1)], s.sent.at[1])
    settle(s.send_b.at[:, pl.ds(0, ndp - 1)], s.sent.at[2])
    settle(s.send_p.at[:, :, pl.ds(0, ndp - 1)], s.sent.at[3])
    settle(s.held.at[:, pl.ds(0, ndp - 1)], s.sent.at[4])
    settle(s.parts.at[:, :, pl.ds(0, ntp - 1)], s.sent.at[5])
    settle(s.land_f.at[:, pl.ds(0, ntp - 1)], s.sent.at[6])


def write_kernel(tok, conv, vec, ssm, tok_out, conv_out, vec_out, ssm_out, sem, ssm_sem):
    layers, rows = ssm.shape[:2]
    for l in range(layers):
        for r in range(rows):
            pltpu.make_async_copy(ssm.at[l, r], ssm_out.at[l, r], ssm_sem).start()
    others = []
    for i, (src, dst) in enumerate(((tok, tok_out), (conv, conv_out), (vec, vec_out))):
        others.append(pltpu.make_async_copy(src, dst, sem.at[i]))
        others[-1].start()
    for copy in others:
        copy.wait()
    pltpu.make_async_copy(ssm, ssm_out, ssm_sem).wait()


VMEM = pl.BlockSpec(memory_space=pltpu.VMEM)
HBM = pl.BlockSpec(memory_space=pl.ANY)


def dma(*shape):
    return pltpu.SemaphoreType.DMA(shape)


SMALLS = (
    "gain", "conv_w", "conv_v", "conv_s", "vec_s", "bias", "decay_log", "skip", "out_gain"
)
INPUTS = ("x_hbm", "w_step_hbm", "w_in_hbm", "w_vec_hbm", "w_out_hbm", "ssm_hbm") + tuple(
    name + "_hbm" for name in SMALLS
)
SCRATCH = (
    "w_step", "w_in", "w_vec", "w_out",
) + SMALLS + (
    "landed", "lhs_buf", "send_a", "land_a", "send_b", "land_b", "send_p", "land_p",
    "read", "drive_pad", "drive_t", "outer", "decay_pad", "decay_t",
    "held", "lhs_out", "parts", "rows", "send_f", "land_f", "land_r",
    "small_sem", "weight_sem", "own_sem", "sent", "got_x", "got_a", "got_b", "got_p", "got_r",
    "got_n", "got_o", "got_f",
)


def shards(
    ntp, ndp, tokens, w_in, w_vec, w_step, conv_weight, conv_vec, conv_state, vec_state,
    ssm_state, step_bias, decay_log, skip_gain, mix_gain, out_gain, w_out,
):
    rows_t, width = tokens.shape
    layers = w_in.shape[0]
    batch = rows_t * ntp
    rows_d = batch // ndp
    cols, vcols = w_in.shape[3], w_vec.shape[3]
    groups = vcols // STATE_DIM
    block = min(cols, 1024)
    chunks = 2 * cols // block
    conv_rows = jnp.transpose(conv_state, (0, 2, 1, 3))
    vec_rows = jnp.transpose(vec_state, (0, 1, 3, 2, 4))
    smalls = (
        mix_gain, conv_weight, conv_vec, conv_rows, vec_rows, step_bias, decay_log, skip_gain,
        out_gain,
    )
    scratch = [pltpu.VMEM(a.shape, a.dtype) for a in (w_step, w_in, w_vec, w_out) + smalls] + [
        pltpu.VMEM((ntp, rows_t, width), BF16),
        pltpu.VMEM((batch, width), F32),
        pltpu.VMEM((layers, ndp, rows_d, vcols), BF16),
        pltpu.VMEM((layers, ndp, rows_d, vcols), BF16),
        pltpu.VMEM((layers, ndp, rows_d, vcols + LANES), BF16),
        pltpu.VMEM((layers, ndp, rows_d, vcols + LANES), BF16),
        pltpu.VMEM((layers, chunks, ndp, rows_d, block), BF16),
        pltpu.VMEM((layers, chunks, ndp, rows_d, block), BF16),
        pltpu.VMEM((rows_d, cols), F32),
        pltpu.VMEM((LANES, cols), F32),
        pltpu.VMEM((cols, LANES), F32),
        pltpu.VMEM((groups, rows_d // 2, LANES, 2 * STATE_DIM), F32),
        pltpu.VMEM((LANES, LANES), F32),
        pltpu.VMEM((LANES, LANES), F32),
        pltpu.VMEM((layers, ndp, rows_d, cols), BF16),
        pltpu.VMEM((batch, cols), F32),
        pltpu.VMEM((layers - 1, 2, ntp, batch, width // 2), BF16),
        pltpu.VMEM((ntp, rows_t, width), BF16),
        pltpu.VMEM((2, ntp, rows_t, width // 2), BF16),
        pltpu.VMEM((2, ntp, rows_t, width // 2), BF16),
        pltpu.VMEM((layers, chunks - 1, rows_d, block), BF16),
        dma(len(SMALLS)), dma(layers, 7), dma(1), dma(len(SEND_KINDS)), dma(1), dma(layers),
        dma(layers), dma(layers, chunks), dma(layers, chunks - 1), dma(layers, chunks // 2),
        dma(layers - 1, 2), dma(1, 2),
    ]
    out_shape = (
        pltpu.VMEM(tokens.shape, BF16),
        pltpu.VMEM(conv_rows.shape, BF16),
        pltpu.VMEM(vec_rows.shape, BF16),
        pltpu.VMEM(ssm_state.shape, F32),
    )
    names = INPUTS + ("tokens", "new_conv", "new_vec", "ssm") + SCRATCH
    results = pl.pallas_call(
        functools.partial(mixer_kernel, ntp, ndp, names),
        out_shape=out_shape,
        in_specs=[HBM] * len(INPUTS),
        out_specs=(VMEM,) * len(out_shape),
        scratch_shapes=scratch,
        compiler_params=pltpu.CompilerParams(
            collective_id=0, has_side_effects=True, vmem_limit_bytes=44 << 20
        ),
    )(tokens, w_step, w_in, w_vec, w_out, ssm_state, *smalls)
    new_tokens, new_conv, new_vec, new_ssm = pl.pallas_call(
        write_kernel,
        out_shape=tuple(jax.ShapeDtypeStruct(r.shape, r.dtype) for r in results),
        in_specs=[VMEM] * 4,
        out_specs=(HBM,) * 4,
        scratch_shapes=[dma(3), pltpu.SemaphoreType.DMA],
        compiler_params=pltpu.CompilerParams(vmem_limit_bytes=8 << 20),
    )(*results)
    return (
        new_tokens,
        jnp.transpose(new_conv, (0, 2, 1, 3)),
        jnp.transpose(new_vec, (0, 1, 3, 2, 4)),
        new_ssm,
    )


def solution(mesh):
    placed = (
        P(("grp", "tp"), "dp"),
        P(None, None, "dp", "tp"),
        P(None, None, "dp", "tp"),
        P(None, "dp", None),
        P(None, None, "tp"),
        P(None, None, None, "tp"),
        P(None, ("grp", "dp"), None, "tp"),
        P(None, None, ("grp", "dp"), None, "tp"),
        P(None, ("grp", "dp"), "tp", None, None),
        P(None, "tp"),
        P(None, "tp"),
        P(None, "tp"),
        P(None, "dp"),
        P(None, "tp"),
        P(None, "tp", "dp"),
    )
    return jax.shard_map(
        functools.partial(shards, mesh.shape["tp"], mesh.shape["dp"]),
        mesh=mesh,
        in_specs=placed,
        out_specs=(
            P(("grp", "tp"), "dp"),
            P(None, ("grp", "dp"), None, "tp"),
            P(None, None, ("grp", "dp"), None, "tp"),
            P(None, ("grp", "dp"), "tp", None, None),
        ),
        check_vma=False,
    )
```

```python
import functools
import types

import jax
import jax.numpy as jnp
from jax import lax
from jax.experimental import pallas as pl
from jax.experimental.pallas import tpu as pltpu
from jax.sharding import PartitionSpec as P

MODEL_WIDTH = 4096
HEAD_DIM = 64
STATE_DIM = 128
LANES = 128
LAYER_COUNT = 2

EPS = 1e-06
F32 = jnp.float32
BF16 = jnp.bfloat16


def remote(src, dst, send_sem, recv_sem, axis, target):
    return pltpu.make_async_remote_copy(
        src_ref=src,
        dst_ref=dst,
        send_sem=send_sem,
        recv_sem=recv_sem,
        device_id={axis: target},
        device_id_type=pl.DeviceIdType.MESH,
    )


def call_out(ntp, ndp):
    barrier = pltpu.get_barrier_semaphore()
    tp, dp = lax.axis_index("tp"), lax.axis_index("dp")

    def call(axis, target):
        pl.semaphore_signal(
            barrier, inc=1, device_id={axis: target}, device_id_type=pl.DeviceIdType.MESH
        )

    @pl.when(dp > 0)
    def _():
        call("dp", dp - 1)

    @pl.when(dp < ndp - 1)
    def _():
        call("dp", dp + 1)

    for k in range(1, ntp):
        call("tp", lax.rem(tp + k, ntp))
    return barrier, ntp - 1 + jnp.asarray(dp > 0, jnp.int32) + jnp.asarray(dp < ndp - 1, jnp.int32)


def pass_word(ndp, know):
    dp = lax.axis_index("dp")

    def tell(side, target):
        pl.semaphore_signal(
            know.at[side], inc=1, device_id={"dp": target}, device_id_type=pl.DeviceIdType.MESH
        )

    @pl.when(jnp.logical_and(dp > 0, dp < ndp - 1))
    def _():
        tell(0, dp - 1)
        tell(1, dp + 1)

    for t in range(ndp - 2):
        @pl.when(dp < ndp - 2 - t)
        def _():
            pl.semaphore_wait(know.at[0], 1)

            @pl.when(dp > 0)
            def _():
                tell(0, dp - 1)

        @pl.when(dp > 1 + t)
        def _():
            pl.semaphore_wait(know.at[1], 1)

            @pl.when(dp < ndp - 1)
            def _():
                tell(1, dp + 1)


def silu(v):
    return v / (1.0 + jnp.exp(-v))


def softplus(v):
    return jnp.maximum(v, 0.0) + jnp.log1p(jnp.exp(-jnp.abs(v)))


def expand(per_head, at, rows):
    per = LANES // HEAD_DIM
    lane = lax.broadcasted_iota(jnp.int32, (rows, LANES), 1)
    out = jnp.broadcast_to(per_head[:, at : at + 1], (rows, LANES))
    for j in range(1, per):
        other = jnp.broadcast_to(per_head[:, at + j : at + j + 1], (rows, LANES))
        out = jnp.where(lane >= j * HEAD_DIM, other, out)
    return out


SEND_KINDS = ("x", "a", "b", "p", "n", "o", "f")


def far_first(me, n):
    low = jnp.asarray(me < (n + 1) // 2, jnp.int32)
    out = []
    for j in range(n - 1):
        up = j + jnp.asarray(j >= me, jnp.int32)
        down = n - 1 - (j + jnp.asarray(j >= n - 1 - me, jnp.int32))
        out.append(low * down + (1 - low) * up)
    return out


def settle(ref, sem):
    pltpu.make_async_copy(ref, ref, sem).wait()


def mixer_kernel(ntp, ndp, names, *refs):
    s = types.SimpleNamespace(**dict(zip(names, refs)))
    rows_t, width = s.tokens.shape
    batch = rows_t * ntp
    rows_d = batch // ndp
    cols = s.w_in.shape[3]
    vcols = s.w_vec.shape[3]
    heads = s.w_step.shape[2]
    local_heads = s.ssm.shape[2]
    groups = vcols // STATE_DIM
    span = cols // groups
    group_heads = local_heads // groups
    block = s.send_p.shape[4]
    blocks = cols // block
    tp = lax.axis_index("tp")
    dp = lax.axis_index("dp")
    far = far_first(dp, ndp)
    relay = ndp == 4
    at_end = jnp.logical_or(dp == 0, dp == ndp - 1)
    inside = jnp.logical_not(at_end)
    across = ndp - 1 - dp

    def load(src, dst, sem):
        copy = pltpu.make_async_copy(src, dst, sem)
        copy.start()
        return copy

    def load_weights(layer):
        vec = [
            load(s.w_vec_hbm.at[layer, role], s.w_vec.at[layer, role], s.weight_sem.at[layer, role])
            for role in (1, 0)
        ]
        step = load(s.w_step_hbm.at[layer], s.w_step.at[layer], s.weight_sem.at[layer, 2])
        return vec, step, [
            load(s.w_in_hbm.at[layer, role], s.w_in.at[layer, role], s.weight_sem.at[layer, 3 + role])
            for role in (1, 0)
        ]

    def load_rest(layer):
        return (
            load(s.ssm_hbm.at[layer], s.ssm.at[layer], s.weight_sem.at[layer, 5]),
            load(s.w_out_hbm.at[layer], s.w_out.at[layer], s.weight_sem.at[layer, 6]),
        )

    barrier, callers = call_out(ntp, ndp)
    load(s.x_hbm, s.landed.at[tp], s.own_sem.at[0]).wait()
    weights = [load_weights(0)]
    smalls = [
        load(getattr(s, name + "_hbm"), getattr(s, name), s.small_sem.at[i])
        for i, name in enumerate(SMALLS)
    ]
    pl.semaphore_wait(barrier, callers)
    for k in range(1, ntp):
        remote(
            s.landed.at[tp], s.landed.at[tp], s.sent.at[0], s.got_x.at[0],
            "tp", lax.rem(tp + k, ntp),
        ).start()
    s.drive_pad[...] = jnp.zeros_like(s.drive_pad)
    s.decay_pad[...] = jnp.zeros_like(s.decay_pad)
    s.outer[...] = jnp.zeros_like(s.outer)
    if relay:
        @pl.when(at_end)
        def _():
            for layer in range(LAYER_COUNT):
                for c in range(2 * blocks - 1):
                    s.land_p[layer, c, across] = jnp.zeros((rows_d, block), BF16)

    pass_word(ndp, s.know)
    for copy in smalls:
        copy.wait()
    settle(s.landed.at[pl.ds(0, ntp - 1)], s.got_x.at[0])
    rest = [load_rest(0)]

    def send_part(layer, c, peer):
        remote(
            s.send_p.at[layer, c, peer], s.land_p.at[layer, c, dp],
            s.sent.at[SEND_KINDS.index("p")], s.got_p.at[layer, c], "dp", peer,
        ).start()

    near = jnp.where(dp == 0, 1, ndp - 2)
    middle = ndp - 1 - near
    side = (dp - 1) * 3

    def deal_relayed(layer, c):
        final = c == 2 * blocks - 1

        @pl.when(at_end)
        def _():
            if not final:
                remote(
                    s.send_p.at[layer, c, across], s.land_r.at[layer, c],
                    s.sent.at[SEND_KINDS.index("p")], s.got_r.at[layer, c], "dp", near,
                ).start()
            else:
                for e in range(c):
                    send_part(layer, e, middle)
                send_part(layer, c, across)
                send_part(layer, c, middle)
                for e in range(c + 1):
                    send_part(layer, e, near)

        @pl.when(inside)
        def _():
            send_part(layer, c, side)
            if not final:
                send_part(layer, c, across)
            else:
                other = 3 - side
                for e in range(c):
                    settle(s.land_r.at[layer, e], s.got_r.at[layer, e])
                    s.send_p[layer, e, other] = (
                        s.send_p[layer, e, other].astype(F32) + s.land_r[layer, e].astype(F32)
                    ).astype(BF16)
                    send_part(layer, e, other)
                send_part(layer, c, other)
                send_part(layer, c, across)

    def project(layer, rows):
        scale_row = s.gain[...].astype(F32)[layer : layer + 1]
        squares = []
        for i in range(ntp):
            part = rows(i)
            squares.append(jnp.sum(part * part, axis=1, keepdims=True))
            s.lhs_buf[i * rows_t : (i + 1) * rows_t, :] = part * scale_row
        squares = jnp.concatenate(squares, axis=0)
        lhs = s.lhs_buf[...].astype(BF16)
        load_vec, load_step, load_in = weights[layer]

        def put(target, at, acc):
            for p in range(ndp):
                target[p, :, at : at + acc.shape[1]] = acc[p * rows_d : (p + 1) * rows_d].astype(
                    BF16
                )

        def deal(target, landing, kind, got):
            for peer in far:
                remote(
                    target.at[peer], landing.at[dp], s.sent.at[SEND_KINDS.index(kind)], got,
                    "dp", peer,
                ).start()

        load_vec[0].wait()
        put(s.send_a.at[layer], 0, jnp.dot(lhs, s.w_vec[layer, 1], preferred_element_type=F32))
        deal(s.send_a.at[layer], s.land_a.at[layer], "a", s.got_a.at[layer])
        load_step.wait()
        load_vec[1].wait()
        small = jnp.dot(lhs, s.w_step[layer], preferred_element_type=F32)
        small = pltpu.roll(small, lax.rem(heads - tp * local_heads, heads), 1)
        lane = lax.broadcasted_iota(jnp.int32, small.shape, 1)
        small = jnp.where(lane == local_heads, jnp.broadcast_to(squares, small.shape), small)
        put(s.send_b.at[layer], vcols, small)
        put(s.send_b.at[layer], 0, jnp.dot(lhs, s.w_vec[layer, 0], preferred_element_type=F32))
        deal(s.send_b.at[layer], s.land_b.at[layer], "b", s.got_b.at[layer])
        for j, role in enumerate((1, 0)):
            load_in[j].wait()
            for b in range(blocks):
                c = j * blocks + b
                acc = jnp.dot(
                    lhs, s.w_in[layer, role, :, b * block : (b + 1) * block],
                    preferred_element_type=F32,
                )
                put(s.send_p.at[layer, c], 0, acc)
                if relay:
                    deal_relayed(layer, c)
                else:
                    deal(s.send_p.at[layer, c], s.land_p.at[layer, c], "p", s.got_p.at[layer, c])

    def total(mine, others):
        acc = mine[dp].astype(F32)
        for k in range(1, ndp):
            acc = acc + others[lax.rem(dp + k, ndp)].astype(F32)
        return acc

    def arrived(landing, got):
        settle(landing.at[pl.ds(0, ndp - 1)], got)

    def arrived_part(layer, c):
        if relay and c < 2 * blocks - 1:
            @pl.when(at_end)
            def _():
                settle(s.land_p.at[layer, c, pl.ds(0, ndp - 2)], s.got_p.at[layer, c])

            @pl.when(inside)
            def _():
                settle(s.land_p.at[layer, c, pl.ds(0, ndp - 1)], s.got_p.at[layer, c])
        else:
            arrived(s.land_p.at[layer, c], s.got_p.at[layer, c])

    def head_step(layer):
        arrived(s.land_a.at[layer], s.got_a.at[layer])
        arrived(s.land_b.at[layer], s.got_b.at[layer])
        small = total(s.send_b.at[layer], s.land_b.at[layer])
        own_sq = small[:, vcols + local_heads : vcols + local_heads + 1]
        scale = lax.rsqrt(own_sq * (1.0 / MODEL_WIDTH) + EPS)
        taps_v = s.conv_v[layer].astype(F32)
        acts = []
        for role in range(2):
            raw = small[:, 0:vcols] if role == 0 else total(s.send_a.at[layer], s.land_a.at[layer])
            fresh = (raw * scale).astype(BF16)
            acc = fresh.astype(F32) * taps_v[role, 3:4]
            for i in range(3):
                acc = acc + s.vec_s[layer, role, i].astype(F32) * taps_v[role, i : i + 1]
            s.new_vec[layer, role, 0] = s.vec_s[layer, role, 1]
            s.new_vec[layer, role, 1] = s.vec_s[layer, role, 2]
            s.new_vec[layer, role, 2] = fresh
            acts.append(silu(acc))
        in_vec, out_vec = acts
        step = softplus(
            small[:, vcols : vcols + local_heads] * scale + s.bias[layer : layer + 1]
        )
        decay = jnp.exp(-step * jnp.exp(s.decay_log[layer : layer + 1]))
        s.decay_pad[0:rows_d, 0:local_heads] = decay
        s.decay_t[...] = jnp.transpose(s.decay_pad[...])
        rest[layer][0].wait()
        row = lax.broadcasted_iota(jnp.int32, (rows_d, STATE_DIM), 0)
        skips = jnp.broadcast_to(s.skip[layer : layer + 1], (rows_d, local_heads))
        inner = []
        for g in range(groups):
            in_g = in_vec[:, g * STATE_DIM : (g + 1) * STATE_DIM]
            out_g = out_vec[:, g * STATE_DIM : (g + 1) * STATE_DIM]
            inner.append(jnp.sum(in_g * out_g, axis=1, keepdims=True))
            acc = jnp.zeros((rows_d, span), F32)
            for r in range(rows_d):
                mine = jnp.where(row == r, out_g, 0.0)
                state = s.ssm[layer, r, g * group_heads : (g + 1) * group_heads]
                acc = acc + lax.dot_general(
                    mine, state.reshape(span, STATE_DIM), (((1,), (1,)), ((), ())),
                    preferred_element_type=F32,
                )
            s.read[:, g * span : (g + 1) * span] = acc
            high = in_g.astype(BF16).astype(F32)
            for r in range(rows_d):
                at = (r % 2) * STATE_DIM
                lanes = slice(at, at + STATE_DIM)
                mine = jnp.where(row == r, high, 0.0)
                s.outer[g, r // 2, 0:rows_d, lanes] = mine
                s.outer[g, r // 2, rows_d : 2 * rows_d, lanes] = mine
                s.outer[g, r // 2, 2 * rows_d : 3 * rows_d, lanes] = jnp.where(
                    row == r, in_g - high, 0.0
                )
        taps = s.conv_w[layer].astype(F32)
        for b in range(blocks):
            arrived_part(layer, b)
            cut = slice(b * block, (b + 1) * block)
            fresh = (total(s.send_p.at[layer, b], s.land_p.at[layer, b]) * scale).astype(BF16)
            acc = fresh.astype(F32) * taps[3:4, cut]
            for i in range(3):
                acc = acc + s.conv_s[layer, i, :, cut].astype(F32) * taps[i : i + 1, cut]
            s.new_conv[layer, 0, :, cut] = s.conv_s[layer, 1, :, cut]
            s.new_conv[layer, 1, :, cut] = s.conv_s[layer, 2, :, cut]
            s.new_conv[layer, 2, :, cut] = fresh
            values = silu(acc)
            for at in range(0, block, LANES):
                lane0 = b * block + at
                head = lane0 // HEAD_DIM
                v = values[:, at : at + LANES]
                drive = expand(step, head, rows_d) * v
                lanes = slice(lane0, lane0 + LANES)
                high = drive.astype(BF16).astype(F32)
                s.drive_pad[0:rows_d, lanes] = high
                s.drive_pad[rows_d : 2 * rows_d, lanes] = drive - high
                s.drive_pad[2 * rows_d : 3 * rows_d, lanes] = high
                s.read[:, lanes] = (
                    expand(decay, head, rows_d) * s.read[:, lanes]
                    + drive * inner[lane0 // span]
                    + expand(skips, head, rows_d) * v
                )
        for at in range(0, cols, LANES):
            s.drive_t[at : at + LANES, :] = jnp.transpose(s.drive_pad[:, at : at + LANES])
        gain_row = s.out_gain[...].astype(F32)[layer : layer + 1]
        for b in range(blocks):
            c = blocks + b
            arrived_part(layer, c)
            fresh = (total(s.send_p.at[layer, c], s.land_p.at[layer, c]) * scale).astype(BF16)
            mixed = s.read[:, b * block : (b + 1) * block] * silu(fresh.astype(F32))
            for at in range(0, block, span):
                cut = slice(b * block + at, b * block + at + span)
                part = mixed[:, at : at + span]
                mean = jnp.mean(part * part, axis=1, keepdims=True)
                s.held[layer, dp, :, cut] = (
                    part * lax.rsqrt(mean + EPS) * gain_row[:, cut]
                ).astype(BF16)
            mine = s.held.at[layer, dp, :, pl.ds(b * block, block)]
            for peer in far:
                remote(
                    mine, mine, s.sent.at[SEND_KINDS.index("n")], s.got_n.at[layer, b], "dp", peer
                ).start()

    def update_state(layer):
        some = min(4, group_heads)

        def some_heads(q, carry):
            first = q * some
            lhs = s.drive_t[pl.ds(pl.multiple_of(first * HEAD_DIM, HEAD_DIM), some * HEAD_DIM), :]
            for pair in range(rows_d // 2):
                added = jnp.dot(
                    lhs, s.outer[first // group_heads, pair], preferred_element_type=F32
                )
                for r in (2 * pair, 2 * pair + 1):
                    at = (r % 2) * STATE_DIM
                    for j in range(some):
                        decay = s.decay_t[pl.ds(first + j, 1), :][:, r : r + 1]
                        s.ssm[layer, r, first + j] = (
                            s.ssm[layer, r, first + j]
                            * jnp.broadcast_to(decay, (HEAD_DIM, STATE_DIM))
                            + added[j * HEAD_DIM : (j + 1) * HEAD_DIM, at : at + STATE_DIM]
                        )
            return carry

        lax.fori_loop(0, local_heads // some, some_heads, 0)

    def gather_out(layer, emit):
        rest[layer][1].wait()
        half = width // 2
        accs = [jnp.zeros((batch, half), F32)] * 2
        for b in range(blocks):
            cut = slice(b * block, (b + 1) * block)
            settle(s.held.at[layer, pl.ds(0, ndp - 1), :, pl.ds(b * block, block)], s.got_n.at[layer, b])
            for i in range(ndp):
                s.lhs_out[i * rows_d : (i + 1) * rows_d, cut] = s.held[layer, i, :, cut].astype(F32)
            lhs = s.lhs_out[:, cut].astype(BF16)
            for h in range(2):
                accs[h] = accs[h] + jnp.dot(
                    lhs, s.w_out[layer, cut, h * half : (h + 1) * half], preferred_element_type=F32
                )
                if b == blocks - 1:
                    emit(h, accs[h])

    project(0, lambda i: s.landed[i].astype(F32))
    for layer in range(LAYER_COUNT):
        last = layer == LAYER_COUNT - 1
        if not last:
            weights.append(load_weights(layer + 1))
            rest.append(load_rest(layer + 1))
        head_step(layer)
        update_state(layer)
        half = width // 2

        def emit(h, acc, layer=layer, last=last):
            kind = s.sent.at[SEND_KINDS.index("f" if last else "o")]
            got = (s.got_f if last else s.got_o).at[0 if last else layer, h]
            if last:
                for i in range(ntp):
                    s.send_f[h, i] = acc[i * rows_t : (i + 1) * rows_t].astype(BF16)
            else:
                s.parts[layer, h, tp] = acc.astype(BF16)
            for k in range(1, ntp):
                peer = lax.rem(tp + k, ntp)
                src = s.send_f.at[h, peer] if last else s.parts.at[layer, h, tp]
                dst = s.land_f.at[h, tp] if last else src
                remote(src, dst, kind, got, "tp", peer).start()

        gather_out(layer, emit)
        if last:
            for h in range(2):
                cut = slice(h * half, (h + 1) * half)
                settle(s.land_f.at[h, pl.ds(0, ntp - 1)], s.got_f.at[0, h])
                s.land_f[h, tp] = s.send_f[h, tp]
                acc = s.rows[tp, :, cut].astype(F32)
                for i in range(ntp):
                    acc = acc + s.land_f[h, i].astype(F32)
                s.tokens[:, cut] = acc.astype(BF16)
        else:
            accs = []
            for h in range(2):
                settle(s.parts.at[layer, h, pl.ds(0, ntp - 1)], s.got_o.at[layer, h])
                acc = s.parts[layer, h, 0].astype(F32)
                for i in range(1, ntp):
                    acc = acc + s.parts[layer, h, i].astype(F32)
                accs.append(acc)
            acc = jnp.concatenate(accs, axis=1)
            before = s.landed if layer == 0 else s.rows

            def rows(i, before=before, acc=acc):
                part = (before[i].astype(F32) + acc[i * rows_t : (i + 1) * rows_t]).astype(BF16)
                s.rows[i] = part
                return part.astype(F32)

            project(layer + 1, rows)
    settle(s.landed.at[pl.ds(0, ntp - 1)], s.sent.at[0])
    settle(s.send_a.at[:, pl.ds(0, ndp - 1)], s.sent.at[1])
    settle(s.send_b.at[:, pl.ds(0, ndp - 1)], s.sent.at[2])
    settle(s.send_p.at[:, :, pl.ds(0, ndp - 1)], s.sent.at[3])
    settle(s.held.at[:, pl.ds(0, ndp - 1)], s.sent.at[4])
    settle(s.parts.at[:, :, pl.ds(0, ntp - 1)], s.sent.at[5])
    settle(s.land_f.at[:, pl.ds(0, ntp - 1)], s.sent.at[6])


def write_kernel(tok, conv, vec, ssm, tok_out, conv_out, vec_out, ssm_out, sem, ssm_sem):
    layers, rows = ssm.shape[:2]
    for l in range(layers):
        for r in range(rows):
            pltpu.make_async_copy(ssm.at[l, r], ssm_out.at[l, r], ssm_sem).start()
    others = []
    for i, (src, dst) in enumerate(((tok, tok_out), (conv, conv_out), (vec, vec_out))):
        others.append(pltpu.make_async_copy(src, dst, sem.at[i]))
        others[-1].start()
    for copy in others:
        copy.wait()
    pltpu.make_async_copy(ssm, ssm_out, ssm_sem).wait()


VMEM = pl.BlockSpec(memory_space=pltpu.VMEM)
HBM = pl.BlockSpec(memory_space=pl.ANY)


def dma(*shape):
    return pltpu.SemaphoreType.DMA(shape)


SMALLS = (
    "gain", "conv_w", "conv_v", "conv_s", "vec_s", "bias", "decay_log", "skip", "out_gain"
)
INPUTS = ("x_hbm", "w_step_hbm", "w_in_hbm", "w_vec_hbm", "w_out_hbm", "ssm_hbm") + tuple(
    name + "_hbm" for name in SMALLS
)
SCRATCH = (
    "w_step", "w_in", "w_vec", "w_out",
) + SMALLS + (
    "landed", "lhs_buf", "send_a", "land_a", "send_b", "land_b", "send_p", "land_p",
    "read", "drive_pad", "drive_t", "outer", "decay_pad", "decay_t",
    "held", "lhs_out", "parts", "rows", "send_f", "land_f", "land_r",
    "small_sem", "weight_sem", "own_sem", "know", "sent", "got_x", "got_a", "got_b", "got_p", "got_r",
    "got_n", "got_o", "got_f",
)


def shards(
    ntp, ndp, tokens, w_in, w_vec, w_step, conv_weight, conv_vec, conv_state, vec_state,
    ssm_state, step_bias, decay_log, skip_gain, mix_gain, out_gain, w_out,
):
    rows_t, width = tokens.shape
    layers = w_in.shape[0]
    batch = rows_t * ntp
    rows_d = batch // ndp
    cols, vcols = w_in.shape[3], w_vec.shape[3]
    groups = vcols // STATE_DIM
    block = min(cols, 1024)
    chunks = 2 * cols // block
    conv_rows = jnp.transpose(conv_state, (0, 2, 1, 3))
    vec_rows = jnp.transpose(vec_state, (0, 1, 3, 2, 4))
    smalls = (
        mix_gain, conv_weight, conv_vec, conv_rows, vec_rows, step_bias, decay_log, skip_gain,
        out_gain,
    )
    scratch = [pltpu.VMEM(a.shape, a.dtype) for a in (w_step, w_in, w_vec, w_out) + smalls] + [
        pltpu.VMEM((ntp, rows_t, width), BF16),
        pltpu.VMEM((batch, width), F32),
        pltpu.VMEM((layers, ndp, rows_d, vcols), BF16),
        pltpu.VMEM((layers, ndp, rows_d, vcols), BF16),
        pltpu.VMEM((layers, ndp, rows_d, vcols + LANES), BF16),
        pltpu.VMEM((layers, ndp, rows_d, vcols + LANES), BF16),
        pltpu.VMEM((layers, chunks, ndp, rows_d, block), BF16),
        pltpu.VMEM((layers, chunks, ndp, rows_d, block), BF16),
        pltpu.VMEM((rows_d, cols), F32),
        pltpu.VMEM((LANES, cols), F32),
        pltpu.VMEM((cols, LANES), F32),
        pltpu.VMEM((groups, rows_d // 2, LANES, 2 * STATE_DIM), F32),
        pltpu.VMEM((LANES, LANES), F32),
        pltpu.VMEM((LANES, LANES), F32),
        pltpu.VMEM((layers, ndp, rows_d, cols), BF16),
        pltpu.VMEM((batch, cols), F32),
        pltpu.VMEM((layers - 1, 2, ntp, batch, width // 2), BF16),
        pltpu.VMEM((ntp, rows_t, width), BF16),
        pltpu.VMEM((2, ntp, rows_t, width // 2), BF16),
        pltpu.VMEM((2, ntp, rows_t, width // 2), BF16),
        pltpu.VMEM((layers, chunks - 1, rows_d, block), BF16),
        dma(len(SMALLS)), dma(layers, 7), dma(1),
        pltpu.SemaphoreType.REGULAR((2,)), dma(len(SEND_KINDS)), dma(1), dma(layers),
        dma(layers), dma(layers, chunks), dma(layers, chunks - 1), dma(layers, chunks // 2),
        dma(layers - 1, 2), dma(1, 2),
    ]
    out_shape = (
        pltpu.VMEM(tokens.shape, BF16),
        pltpu.VMEM(conv_rows.shape, BF16),
        pltpu.VMEM(vec_rows.shape, BF16),
        pltpu.VMEM(ssm_state.shape, F32),
    )
    names = INPUTS + ("tokens", "new_conv", "new_vec", "ssm") + SCRATCH
    results = pl.pallas_call(
        functools.partial(mixer_kernel, ntp, ndp, names),
        out_shape=out_shape,
        in_specs=[HBM] * len(INPUTS),
        out_specs=(VMEM,) * len(out_shape),
        scratch_shapes=scratch,
        compiler_params=pltpu.CompilerParams(
            collective_id=0, has_side_effects=True, vmem_limit_bytes=44 << 20
        ),
    )(tokens, w_step, w_in, w_vec, w_out, ssm_state, *smalls)
    new_tokens, new_conv, new_vec, new_ssm = pl.pallas_call(
        write_kernel,
        out_shape=tuple(jax.ShapeDtypeStruct(r.shape, r.dtype) for r in results),
        in_specs=[VMEM] * 4,
        out_specs=(HBM,) * 4,
        scratch_shapes=[dma(3), pltpu.SemaphoreType.DMA],
        compiler_params=pltpu.CompilerParams(vmem_limit_bytes=8 << 20),
    )(*results)
    return (
        new_tokens,
        jnp.transpose(new_conv, (0, 2, 1, 3)),
        jnp.transpose(new_vec, (0, 1, 3, 2, 4)),
        new_ssm,
    )


def solution(mesh):
    placed = (
        P(("grp", "tp"), "dp"),
        P(None, None, "dp", "tp"),
        P(None, None, "dp", "tp"),
        P(None, "dp", None),
        P(None, None, "tp"),
        P(None, None, None, "tp"),
        P(None, ("grp", "dp"), None, "tp"),
        P(None, None, ("grp", "dp"), None, "tp"),
        P(None, ("grp", "dp"), "tp", None, None),
        P(None, "tp"),
        P(None, "tp"),
        P(None, "tp"),
        P(None, "dp"),
        P(None, "tp"),
        P(None, "tp", "dp"),
    )
    return jax.shard_map(
        functools.partial(shards, mesh.shape["tp"], mesh.shape["dp"]),
        mesh=mesh,
        in_specs=placed,
        out_specs=(
            P(("grp", "tp"), "dp"),
            P(None, ("grp", "dp"), None, "tp"),
            P(None, None, ("grp", "dp"), None, "tp"),
            P(None, ("grp", "dp"), "tp", None, None),
        ),
        check_vma=False,
    )
```

```python
import functools
import types

import jax
import jax.numpy as jnp
from jax import lax
from jax.experimental import pallas as pl
from jax.experimental.pallas import tpu as pltpu
from jax.sharding import PartitionSpec as P

MODEL_WIDTH = 4096
HEAD_DIM = 64
STATE_DIM = 128
LANES = 128
LAYER_COUNT = 2

EPS = 1e-06
F32 = jnp.float32
BF16 = jnp.bfloat16


def remote(src, dst, send_sem, recv_sem, axis, target):
    return pltpu.make_async_remote_copy(
        src_ref=src,
        dst_ref=dst,
        send_sem=send_sem,
        recv_sem=recv_sem,
        device_id={axis: target},
        device_id_type=pl.DeviceIdType.MESH,
    )


def call_out(ntp, ndp):
    barrier = pltpu.get_barrier_semaphore()
    tp, dp = lax.axis_index("tp"), lax.axis_index("dp")

    def call(axis, target):
        pl.semaphore_signal(
            barrier, inc=1, device_id={axis: target}, device_id_type=pl.DeviceIdType.MESH
        )

    @pl.when(dp > 0)
    def _():
        call("dp", dp - 1)

    @pl.when(dp < ndp - 1)
    def _():
        call("dp", dp + 1)

    for k in range(1, ntp):
        call("tp", lax.rem(tp + k, ntp))
    return barrier, ntp - 1 + jnp.asarray(dp > 0, jnp.int32) + jnp.asarray(dp < ndp - 1, jnp.int32)


def learn_one(ndp, know):
    dp = lax.axis_index("dp")

    @pl.when(dp == 0)
    def _():
        pl.semaphore_wait(know.at[0], 1)

    @pl.when(dp == ndp - 1)
    def _():
        pl.semaphore_wait(know.at[1], 1)


def pass_word(ndp, know, ends):
    dp = lax.axis_index("dp")

    def tell(side, target):
        pl.semaphore_signal(
            know.at[side], inc=1, device_id={"dp": target}, device_id_type=pl.DeviceIdType.MESH
        )

    @pl.when(jnp.logical_and(dp > 0, dp < ndp - 1))
    def _():
        tell(0, dp - 1)
        tell(1, dp + 1)

    for t in range(ndp - 2):
        if not ends:
            @pl.when(jnp.logical_and(dp > 0, dp < ndp - 2 - t))
            def _():
                pl.semaphore_wait(know.at[0], 1)
                tell(0, dp - 1)

            @pl.when(jnp.logical_and(dp > 1 + t, dp < ndp - 1))
            def _():
                pl.semaphore_wait(know.at[1], 1)
                tell(1, dp + 1)

            continue

        @pl.when(dp < ndp - 2 - t)
        def _():
            pl.semaphore_wait(know.at[0], 1)

            @pl.when(dp > 0)
            def _():
                tell(0, dp - 1)

        @pl.when(dp > 1 + t)
        def _():
            pl.semaphore_wait(know.at[1], 1)

            @pl.when(dp < ndp - 1)
            def _():
                tell(1, dp + 1)


def silu(v):
    return v / (1.0 + jnp.exp(-v))


def softplus(v):
    return jnp.maximum(v, 0.0) + jnp.log1p(jnp.exp(-jnp.abs(v)))


def expand(per_head, at, rows):
    per = LANES // HEAD_DIM
    lane = lax.broadcasted_iota(jnp.int32, (rows, LANES), 1)
    out = jnp.broadcast_to(per_head[:, at : at + 1], (rows, LANES))
    for j in range(1, per):
        other = jnp.broadcast_to(per_head[:, at + j : at + j + 1], (rows, LANES))
        out = jnp.where(lane >= j * HEAD_DIM, other, out)
    return out


SEND_KINDS = ("x", "a", "b", "p", "n", "o", "f")


def far_first(me, n):
    low = jnp.asarray(me < (n + 1) // 2, jnp.int32)
    out = []
    for j in range(n - 1):
        up = j + jnp.asarray(j >= me, jnp.int32)
        down = n - 1 - (j + jnp.asarray(j >= n - 1 - me, jnp.int32))
        out.append(low * down + (1 - low) * up)
    return out


def settle(ref, sem):
    pltpu.make_async_copy(ref, ref, sem).wait()


def mixer_kernel(ntp, ndp, names, *refs):
    s = types.SimpleNamespace(**dict(zip(names, refs)))
    rows_t, width = s.tokens.shape
    batch = rows_t * ntp
    rows_d = batch // ndp
    cols = s.w_in.shape[3]
    vcols = s.w_vec.shape[3]
    heads = s.w_step.shape[2]
    local_heads = s.ssm.shape[2]
    groups = vcols // STATE_DIM
    span = cols // groups
    group_heads = local_heads // groups
    block = s.send_p.shape[4]
    blocks = cols // block
    tp = lax.axis_index("tp")
    dp = lax.axis_index("dp")
    far = far_first(dp, ndp)
    relay = ndp == 4
    at_end = jnp.logical_or(dp == 0, dp == ndp - 1)
    inside = jnp.logical_not(at_end)
    across = ndp - 1 - dp

    def load(src, dst, sem):
        copy = pltpu.make_async_copy(src, dst, sem)
        copy.start()
        return copy

    def load_weights(layer):
        vec = [
            load(s.w_vec_hbm.at[layer, role], s.w_vec.at[layer, role], s.weight_sem.at[role])
            for role in (1, 0)
        ]
        step = load(s.w_step_hbm.at[layer], s.w_step.at[layer], s.weight_sem.at[2])
        return vec, step, [
            load(s.w_in_hbm.at[layer, role], s.w_in.at[layer, role], s.weight_sem.at[3 + role])
            for role in (1, 0)
        ]

    def load_rest(layer):
        return (
            load(s.ssm_hbm.at[layer], s.ssm.at[layer], s.rest_sem.at[layer, 0]),
            load(s.w_out_hbm.at[layer], s.w_out.at[layer], s.rest_sem.at[layer, 1]),
        )

    barrier, callers = call_out(ntp, ndp)
    own = load(s.x_hbm, s.landed.at[tp], s.own_sem.at[0])
    smalls = [load(s.gain_hbm, s.gain, s.small_sem.at[0])]
    own.wait()
    weights = [load_weights(0)]
    smalls += [
        load(getattr(s, name + "_hbm"), getattr(s, name), s.small_sem.at[i])
        for i, name in enumerate(SMALLS) if i
    ]
    pl.semaphore_wait(barrier, callers)
    for k in range(1, ntp):
        remote(
            s.landed.at[tp], s.landed.at[tp], s.sent.at[0], s.got_x.at[0],
            "tp", lax.rem(tp + k, ntp),
        ).start()
    s.drive_pad[...] = jnp.zeros_like(s.drive_pad)
    s.decay_pad[...] = jnp.zeros_like(s.decay_pad)
    s.outer[...] = jnp.zeros_like(s.outer)
    if relay:
        @pl.when(at_end)
        def _():
            for layer in range(LAYER_COUNT):
                for c in range(2 * blocks - 1):
                    s.land_p[layer, c, across] = jnp.zeros((rows_d, block), BF16)

    pass_word(ndp, s.know, not relay)
    smalls[0].wait()
    settle(s.landed.at[pl.ds(0, ntp - 1)], s.got_x.at[0])
    rest = [load_rest(0)]

    def send_part(layer, c, peer):
        remote(
            s.send_p.at[layer, c, peer], s.land_p.at[layer, c, dp],
            s.sent.at[SEND_KINDS.index("p")], s.got_p.at[layer, c], "dp", peer,
        ).start()

    near = jnp.where(dp == 0, 1, ndp - 2)
    middle = ndp - 1 - near
    side = (dp - 1) * 3

    def deal_relayed(layer, c):
        final = c == 2 * blocks - 1

        @pl.when(at_end)
        def _():
            if not final:
                remote(
                    s.send_p.at[layer, c, across], s.land_r.at[layer, c],
                    s.sent.at[SEND_KINDS.index("p")], s.got_r.at[layer, c], "dp", near,
                ).start()
            else:
                for e in range(c):
                    send_part(layer, e, middle)
                send_part(layer, c, across)
                send_part(layer, c, middle)
                for e in range(c + 1):
                    send_part(layer, e, near)

        @pl.when(inside)
        def _():
            send_part(layer, c, side)
            if not final:
                send_part(layer, c, across)
            else:
                other = 3 - side
                for e in range(c):
                    settle(s.land_r.at[layer, e], s.got_r.at[layer, e])
                    s.send_p[layer, e, other] = (
                        s.send_p[layer, e, other].astype(F32) + s.land_r[layer, e].astype(F32)
                    ).astype(BF16)
                    send_part(layer, e, other)
                send_part(layer, c, other)
                send_part(layer, c, across)

    def project(layer, rows):
        scale_row = s.gain[...].astype(F32)[layer : layer + 1]
        squares = []
        for i in range(ntp):
            part = rows(i)
            squares.append(jnp.sum(part * part, axis=1, keepdims=True))
            s.lhs_buf[i * rows_t : (i + 1) * rows_t, :] = part * scale_row
        squares = jnp.concatenate(squares, axis=0)
        lhs = s.lhs_buf[...].astype(BF16)
        load_vec, load_step, load_in = weights[layer]

        def put(target, at, acc):
            for p in range(ndp):
                target[p, :, at : at + acc.shape[1]] = acc[p * rows_d : (p + 1) * rows_d].astype(
                    BF16
                )

        def deal(target, landing, kind, got, peers=far):
            for peer in peers:
                remote(
                    target.at[peer], landing.at[dp], s.sent.at[SEND_KINDS.index(kind)], got,
                    "dp", peer,
                ).start()

        def deal_small(kind, target, landing, got):
            args = (target.at[layer], landing.at[layer], kind, got.at[layer])
            if relay:
                @pl.when(at_end)
                def _():
                    deal(*args, (middle,) if layer == 0 else (across, middle))

                @pl.when(inside)
                def _():
                    deal(*args)
            else:
                deal(*args)
            return args

        load_vec[0].wait()
        put(s.send_a.at[layer], 0, jnp.dot(lhs, s.w_vec[layer, 1], preferred_element_type=F32))
        if relay and layer == 0:
            learn_one(ndp, s.know)
        late = [deal_small("a", s.send_a, s.land_a, s.got_a)]
        load_step.wait()
        load_vec[1].wait()
        small = jnp.dot(lhs, s.w_step[layer], preferred_element_type=F32)
        small = pltpu.roll(small, lax.rem(heads - tp * local_heads, heads), 1)
        lane = lax.broadcasted_iota(jnp.int32, small.shape, 1)
        small = jnp.where(lane == local_heads, jnp.broadcast_to(squares, small.shape), small)
        put(s.send_b.at[layer], vcols, small)
        put(s.send_b.at[layer], 0, jnp.dot(lhs, s.w_vec[layer, 0], preferred_element_type=F32))
        late.append(deal_small("b", s.send_b, s.land_b, s.got_b))
        for j, role in enumerate((1, 0)):
            load_in[j].wait()
            for b in range(blocks):
                c = j * blocks + b
                acc = jnp.dot(
                    lhs, s.w_in[layer, role, :, b * block : (b + 1) * block],
                    preferred_element_type=F32,
                )
                put(s.send_p.at[layer, c], 0, acc)
                if relay:
                    deal_relayed(layer, c)
                    if layer == 0 and c == blocks - 1:
                        learn_one(ndp, s.know)

                        @pl.when(at_end)
                        def _():
                            for args in late:
                                deal(*args, (across,))

                    if c == 2 * blocks - 2:
                        @pl.when(at_end)
                        def _():
                            for args in late:
                                deal(*args, (near,))

                else:
                    deal(s.send_p.at[layer, c], s.land_p.at[layer, c], "p", s.got_p.at[layer, c])

    def total(mine, others):
        acc = mine[dp].astype(F32)
        for k in range(1, ndp):
            acc = acc + others[lax.rem(dp + k, ndp)].astype(F32)
        return acc

    def arrived(landing, got):
        settle(landing.at[pl.ds(0, ndp - 1)], got)

    def arrived_part(layer, c):
        if relay and c < 2 * blocks - 1:
            @pl.when(at_end)
            def _():
                settle(s.land_p.at[layer, c, pl.ds(0, ndp - 2)], s.got_p.at[layer, c])

            @pl.when(inside)
            def _():
                settle(s.land_p.at[layer, c, pl.ds(0, ndp - 1)], s.got_p.at[layer, c])
        else:
            arrived(s.land_p.at[layer, c], s.got_p.at[layer, c])

    def head_step(layer):
        if layer == 0:
            for copy in smalls[1:]:
                copy.wait()
        arrived(s.land_a.at[layer], s.got_a.at[layer])
        arrived(s.land_b.at[layer], s.got_b.at[layer])
        small = total(s.send_b.at[layer], s.land_b.at[layer])
        own_sq = small[:, vcols + local_heads : vcols + local_heads + 1]
        scale = lax.rsqrt(own_sq * (1.0 / MODEL_WIDTH) + EPS)
        taps_v = s.conv_v[layer].astype(F32)
        acts = []
        for role in range(2):
            raw = small[:, 0:vcols] if role == 0 else total(s.send_a.at[layer], s.land_a.at[layer])
            fresh = (raw * scale).astype(BF16)
            acc = fresh.astype(F32) * taps_v[role, 3:4]
            for i in range(3):
                acc = acc + s.vec_s[layer, role, i].astype(F32) * taps_v[role, i : i + 1]
            s.new_vec[layer, role, 0] = s.vec_s[layer, role, 1]
            s.new_vec[layer, role, 1] = s.vec_s[layer, role, 2]
            s.new_vec[layer, role, 2] = fresh
            acts.append(silu(acc))
        in_vec, out_vec = acts
        step = softplus(
            small[:, vcols : vcols + local_heads] * scale + s.bias[layer : layer + 1]
        )
        decay = jnp.exp(-step * jnp.exp(s.decay_log[layer : layer + 1]))
        s.decay_pad[0:rows_d, 0:local_heads] = decay
        s.decay_t[...] = jnp.transpose(s.decay_pad[...])
        rest[layer][0].wait()
        row = lax.broadcasted_iota(jnp.int32, (rows_d, STATE_DIM), 0)
        skips = jnp.broadcast_to(s.skip[layer : layer + 1], (rows_d, local_heads))
        inner = []
        for g in range(groups):
            in_g = in_vec[:, g * STATE_DIM : (g + 1) * STATE_DIM]
            out_g = out_vec[:, g * STATE_DIM : (g + 1) * STATE_DIM]
            inner.append(jnp.sum(in_g * out_g, axis=1, keepdims=True))
            acc = jnp.zeros((rows_d, span), F32)
            for r in range(rows_d):
                mine = jnp.where(row == r, out_g, 0.0)
                state = s.ssm[layer, r, g * group_heads : (g + 1) * group_heads]
                acc = acc + lax.dot_general(
                    mine, state.reshape(span, STATE_DIM), (((1,), (1,)), ((), ())),
                    preferred_element_type=F32,
                )
            s.read[:, g * span : (g + 1) * span] = acc
            high = in_g.astype(BF16).astype(F32)
            for r in range(rows_d):
                at = (r % 2) * STATE_DIM
                lanes = slice(at, at + STATE_DIM)
                mine = jnp.where(row == r, high, 0.0)
                s.outer[g, r // 2, 0:rows_d, lanes] = mine
                s.outer[g, r // 2, rows_d : 2 * rows_d, lanes] = mine
                s.outer[g, r // 2, 2 * rows_d : 3 * rows_d, lanes] = jnp.where(
                    row == r, in_g - high, 0.0
                )
        taps = s.conv_w[layer].astype(F32)
        for b in range(blocks):
            arrived_part(layer, b)
            cut = slice(b * block, (b + 1) * block)
            fresh = (total(s.send_p.at[layer, b], s.land_p.at[layer, b]) * scale).astype(BF16)
            acc = fresh.astype(F32) * taps[3:4, cut]
            for i in range(3):
                acc = acc + s.conv_s[layer, i, :, cut].astype(F32) * taps[i : i + 1, cut]
            s.new_conv[layer, 0, :, cut] = s.conv_s[layer, 1, :, cut]
            s.new_conv[layer, 1, :, cut] = s.conv_s[layer, 2, :, cut]
            s.new_conv[layer, 2, :, cut] = fresh
            values = silu(acc)
            for at in range(0, block, LANES):
                lane0 = b * block + at
                head = lane0 // HEAD_DIM
                v = values[:, at : at + LANES]
                drive = expand(step, head, rows_d) * v
                lanes = slice(lane0, lane0 + LANES)
                high = drive.astype(BF16).astype(F32)
                s.drive_pad[0:rows_d, lanes] = high
                s.drive_pad[rows_d : 2 * rows_d, lanes] = drive - high
                s.drive_pad[2 * rows_d : 3 * rows_d, lanes] = high
                s.read[:, lanes] = (
                    expand(decay, head, rows_d) * s.read[:, lanes]
                    + drive * inner[lane0 // span]
                    + expand(skips, head, rows_d) * v
                )
        gain_row = s.out_gain[...].astype(F32)[layer : layer + 1]
        for b in range(blocks):
            c = blocks + b
            arrived_part(layer, c)
            fresh = (total(s.send_p.at[layer, c], s.land_p.at[layer, c]) * scale).astype(BF16)
            mixed = s.read[:, b * block : (b + 1) * block] * silu(fresh.astype(F32))
            for at in range(0, block, span):
                cut = slice(b * block + at, b * block + at + span)
                part = mixed[:, at : at + span]
                mean = jnp.mean(part * part, axis=1, keepdims=True)
                s.held[layer, dp, :, cut] = (
                    part * lax.rsqrt(mean + EPS) * gain_row[:, cut]
                ).astype(BF16)
                g = (b * block + at) // span
                mine = s.held.at[layer, dp, :, pl.ds(g * span, span)]
                for peer in far:
                    remote(
                        mine, mine, s.sent.at[SEND_KINDS.index("n")], s.got_n.at[layer, g],
                        "dp", peer,
                    ).start()

    def update_state(layer, half):
        some = min(4, group_heads)
        for at in range(half * cols // 2, (half + 1) * cols // 2, LANES):
            s.drive_t[at : at + LANES, :] = jnp.transpose(s.drive_pad[:, at : at + LANES])

        def some_heads(q, carry):
            first = q * some
            lhs = s.drive_t[pl.ds(pl.multiple_of(first * HEAD_DIM, HEAD_DIM), some * HEAD_DIM), :]
            for pair in range(rows_d // 2):
                added = jnp.dot(
                    lhs, s.outer[first // group_heads, pair], preferred_element_type=F32
                )
                for r in (2 * pair, 2 * pair + 1):
                    at = (r % 2) * STATE_DIM
                    for j in range(some):
                        decay = s.decay_t[pl.ds(first + j, 1), :][:, r : r + 1]
                        s.ssm[layer, r, first + j] = (
                            s.ssm[layer, r, first + j]
                            * jnp.broadcast_to(decay, (HEAD_DIM, STATE_DIM))
                            + added[j * HEAD_DIM : (j + 1) * HEAD_DIM, at : at + STATE_DIM]
                        )
            return carry

        steps = local_heads // some
        lax.fori_loop(half * steps // 2, (half + 1) * steps // 2, some_heads, 0)

    def gather_out(layer, emit):
        rest[layer][1].wait()
        half = width // 2
        accs = [jnp.zeros((batch, half), F32)] * 2
        for g in range(groups):
            cut = slice(g * span, (g + 1) * span)
            settle(s.held.at[layer, pl.ds(0, ndp - 1), :, pl.ds(g * span, span)], s.got_n.at[layer, g])
            for i in range(ndp):
                s.lhs_out[i * rows_d : (i + 1) * rows_d, cut] = s.held[layer, i, :, cut].astype(F32)
            lhs = s.lhs_out[:, cut].astype(BF16)
            for h in range(2):
                accs[h] = accs[h] + jnp.dot(
                    lhs, s.w_out[layer, cut, h * half : (h + 1) * half], preferred_element_type=F32
                )
                if g == groups - 1:
                    emit(h, accs[h])

    project(0, lambda i: s.landed[i].astype(F32))
    for layer in range(LAYER_COUNT):
        last = layer == LAYER_COUNT - 1
        if not last:
            weights.append(load_weights(layer + 1))
            rest.append(load_rest(layer + 1))
        head_step(layer)
        update_state(layer, 0)
        half = width // 2

        def emit(h, acc, layer=layer, last=last):
            kind = s.sent.at[SEND_KINDS.index("f" if last else "o")]
            got = (s.got_f if last else s.got_o).at[0 if last else layer, h]
            if last:
                for i in range(ntp):
                    s.send_f[h, i] = acc[i * rows_t : (i + 1) * rows_t].astype(BF16)
            else:
                s.parts[layer, h, tp] = acc.astype(BF16)
            for k in range(1, ntp):
                peer = lax.rem(tp + k, ntp)
                src = s.send_f.at[h, peer] if last else s.parts.at[layer, h, tp]
                dst = s.land_f.at[h, tp] if last else src
                remote(src, dst, kind, got, "tp", peer).start()

        gather_out(layer, emit)
        update_state(layer, 1)
        if last:
            for h in range(2):
                cut = slice(h * half, (h + 1) * half)
                settle(s.land_f.at[h, pl.ds(0, ntp - 1)], s.got_f.at[0, h])
                s.land_f[h, tp] = s.send_f[h, tp]
                acc = s.rows[tp, :, cut].astype(F32)
                for i in range(ntp):
                    acc = acc + s.land_f[h, i].astype(F32)
                s.tokens[:, cut] = acc.astype(BF16)
        else:
            accs = []
            for h in range(2):
                settle(s.parts.at[layer, h, pl.ds(0, ntp - 1)], s.got_o.at[layer, h])
                acc = s.parts[layer, h, 0].astype(F32)
                for i in range(1, ntp):
                    acc = acc + s.parts[layer, h, i].astype(F32)
                accs.append(acc)
            acc = jnp.concatenate(accs, axis=1)
            before = s.landed if layer == 0 else s.rows

            def rows(i, before=before, acc=acc):
                part = (before[i].astype(F32) + acc[i * rows_t : (i + 1) * rows_t]).astype(BF16)
                s.rows[i] = part
                return part.astype(F32)

            project(layer + 1, rows)
    settle(s.landed.at[pl.ds(0, ntp - 1)], s.sent.at[0])
    settle(s.send_a.at[:, pl.ds(0, ndp - 1)], s.sent.at[1])
    settle(s.send_b.at[:, pl.ds(0, ndp - 1)], s.sent.at[2])
    settle(s.send_p.at[:, :, pl.ds(0, ndp - 1)], s.sent.at[3])
    settle(s.held.at[:, pl.ds(0, ndp - 1)], s.sent.at[4])
    settle(s.parts.at[:, :, pl.ds(0, ntp - 1)], s.sent.at[5])
    settle(s.land_f.at[:, pl.ds(0, ntp - 1)], s.sent.at[6])


def write_kernel(tok, conv, vec, ssm, tok_out, conv_out, vec_out, ssm_out, sem, ssm_sem):
    layers, rows = ssm.shape[:2]
    for l in range(layers):
        for r in range(rows):
            pltpu.make_async_copy(ssm.at[l, r], ssm_out.at[l, r], ssm_sem).start()
    others = []
    for i, (src, dst) in enumerate(((tok, tok_out), (conv, conv_out), (vec, vec_out))):
        others.append(pltpu.make_async_copy(src, dst, sem.at[i]))
        others[-1].start()
    for copy in others:
        copy.wait()
    pltpu.make_async_copy(ssm, ssm_out, ssm_sem).wait()


VMEM = pl.BlockSpec(memory_space=pltpu.VMEM)
HBM = pl.BlockSpec(memory_space=pl.ANY)


def dma(*shape):
    return pltpu.SemaphoreType.DMA(shape)


SMALLS = (
    "gain", "conv_w", "conv_v", "conv_s", "vec_s", "bias", "decay_log", "skip", "out_gain"
)
INPUTS = ("x_hbm", "w_step_hbm", "w_in_hbm", "w_vec_hbm", "w_out_hbm", "ssm_hbm") + tuple(
    name + "_hbm" for name in SMALLS
)
SCRATCH = (
    "w_step", "w_in", "w_vec", "w_out",
) + SMALLS + (
    "landed", "lhs_buf", "send_a", "land_a", "send_b", "land_b", "send_p", "land_p",
    "read", "drive_pad", "drive_t", "outer", "decay_pad", "decay_t",
    "held", "lhs_out", "parts", "rows", "send_f", "land_f", "land_r",
    "small_sem", "weight_sem", "rest_sem", "own_sem", "know", "sent", "got_x", "got_a", "got_b", "got_p", "got_r",
    "got_n", "got_o", "got_f",
)


def shards(
    ntp, ndp, tokens, w_in, w_vec, w_step, conv_weight, conv_vec, conv_state, vec_state,
    ssm_state, step_bias, decay_log, skip_gain, mix_gain, out_gain, w_out,
):
    rows_t, width = tokens.shape
    layers = w_in.shape[0]
    batch = rows_t * ntp
    rows_d = batch // ndp
    cols, vcols = w_in.shape[3], w_vec.shape[3]
    groups = vcols // STATE_DIM
    block = min(cols, 1024)
    chunks = 2 * cols // block
    conv_rows = jnp.transpose(conv_state, (0, 2, 1, 3))
    vec_rows = jnp.transpose(vec_state, (0, 1, 3, 2, 4))
    smalls = (
        mix_gain, conv_weight, conv_vec, conv_rows, vec_rows, step_bias, decay_log, skip_gain,
        out_gain,
    )
    scratch = [pltpu.VMEM(a.shape, a.dtype) for a in (w_step, w_in, w_vec, w_out) + smalls] + [
        pltpu.VMEM((ntp, rows_t, width), BF16),
        pltpu.VMEM((batch, width), F32),
        pltpu.VMEM((layers, ndp, rows_d, vcols), BF16),
        pltpu.VMEM((layers, ndp, rows_d, vcols), BF16),
        pltpu.VMEM((layers, ndp, rows_d, vcols + LANES), BF16),
        pltpu.VMEM((layers, ndp, rows_d, vcols + LANES), BF16),
        pltpu.VMEM((layers, chunks, ndp, rows_d, block), BF16),
        pltpu.VMEM((layers, chunks, ndp, rows_d, block), BF16),
        pltpu.VMEM((rows_d, cols), F32),
        pltpu.VMEM((LANES, cols), F32),
        pltpu.VMEM((cols, LANES), F32),
        pltpu.VMEM((groups, rows_d // 2, LANES, 2 * STATE_DIM), F32),
        pltpu.VMEM((LANES, LANES), F32),
        pltpu.VMEM((LANES, LANES), F32),
        pltpu.VMEM((layers, ndp, rows_d, cols), BF16),
        pltpu.VMEM((batch, cols), F32),
        pltpu.VMEM((layers - 1, 2, ntp, batch, width // 2), BF16),
        pltpu.VMEM((ntp, rows_t, width), BF16),
        pltpu.VMEM((2, ntp, rows_t, width // 2), BF16),
        pltpu.VMEM((2, ntp, rows_t, width // 2), BF16),
        pltpu.VMEM((layers, chunks - 1, rows_d, block), BF16),
        dma(len(SMALLS)), dma(5), dma(layers, 2), dma(1),
        pltpu.SemaphoreType.REGULAR((2,)), dma(len(SEND_KINDS)), dma(1), dma(layers),
        dma(layers), dma(layers, chunks), dma(layers, chunks - 1), dma(layers, groups),
        dma(layers - 1, 2), dma(1, 2),
    ]
    out_shape = (
        pltpu.VMEM(tokens.shape, BF16),
        pltpu.VMEM(conv_rows.shape, BF16),
        pltpu.VMEM(vec_rows.shape, BF16),
        pltpu.VMEM(ssm_state.shape, F32),
    )
    names = INPUTS + ("tokens", "new_conv", "new_vec", "ssm") + SCRATCH
    results = pl.pallas_call(
        functools.partial(mixer_kernel, ntp, ndp, names),
        out_shape=out_shape,
        in_specs=[HBM] * len(INPUTS),
        out_specs=(VMEM,) * len(out_shape),
        scratch_shapes=scratch,
        compiler_params=pltpu.CompilerParams(
            collective_id=0, has_side_effects=True, vmem_limit_bytes=44 << 20
        ),
    )(tokens, w_step, w_in, w_vec, w_out, ssm_state, *smalls)
    new_tokens, new_conv, new_vec, new_ssm = pl.pallas_call(
        write_kernel,
        out_shape=tuple(jax.ShapeDtypeStruct(r.shape, r.dtype) for r in results),
        in_specs=[VMEM] * 4,
        out_specs=(HBM,) * 4,
        scratch_shapes=[dma(3), pltpu.SemaphoreType.DMA],
        compiler_params=pltpu.CompilerParams(vmem_limit_bytes=8 << 20),
    )(*results)
    return (
        new_tokens,
        jnp.transpose(new_conv, (0, 2, 1, 3)),
        jnp.transpose(new_vec, (0, 1, 3, 2, 4)),
        new_ssm,
    )


def solution(mesh):
    placed = (
        P(("grp", "tp"), "dp"),
        P(None, None, "dp", "tp"),
        P(None, None, "dp", "tp"),
        P(None, "dp", None),
        P(None, None, "tp"),
        P(None, None, None, "tp"),
        P(None, ("grp", "dp"), None, "tp"),
        P(None, None, ("grp", "dp"), None, "tp"),
        P(None, ("grp", "dp"), "tp", None, None),
        P(None, "tp"),
        P(None, "tp"),
        P(None, "tp"),
        P(None, "dp"),
        P(None, "tp"),
        P(None, "tp", "dp"),
    )
    return jax.shard_map(
        functools.partial(shards, mesh.shape["tp"], mesh.shape["dp"]),
        mesh=mesh,
        in_specs=placed,
        out_specs=(
            P(("grp", "tp"), "dp"),
            P(None, ("grp", "dp"), None, "tp"),
            P(None, None, ("grp", "dp"), None, "tp"),
            P(None, ("grp", "dp"), "tp", None, None),
        ),
        check_vma=False,
    )
```

```python
import functools
import types

import jax
import jax.numpy as jnp
from jax import lax
from jax.experimental import pallas as pl
from jax.experimental.pallas import tpu as pltpu
from jax.sharding import PartitionSpec as P

MODEL_WIDTH = 4096
HEAD_DIM = 64
STATE_DIM = 128
LANES = 128
LAYER_COUNT = 2

EPS = 1e-06
F32 = jnp.float32
BF16 = jnp.bfloat16


def remote(src, dst, send_sem, recv_sem, axis, target):
    return pltpu.make_async_remote_copy(
        src_ref=src,
        dst_ref=dst,
        send_sem=send_sem,
        recv_sem=recv_sem,
        device_id={axis: target},
        device_id_type=pl.DeviceIdType.MESH,
    )


def call_out(ntp, ndp):
    barrier = pltpu.get_barrier_semaphore()
    tp, dp = lax.axis_index("tp"), lax.axis_index("dp")

    def call(axis, target):
        pl.semaphore_signal(
            barrier, inc=1, device_id={axis: target}, device_id_type=pl.DeviceIdType.MESH
        )

    @pl.when(dp > 0)
    def _():
        call("dp", dp - 1)

    @pl.when(dp < ndp - 1)
    def _():
        call("dp", dp + 1)

    for k in range(1, ntp):
        call("tp", lax.rem(tp + k, ntp))
    return barrier, ntp - 1 + jnp.asarray(dp > 0, jnp.int32) + jnp.asarray(dp < ndp - 1, jnp.int32)


def learn_one(ndp, know):
    dp = lax.axis_index("dp")

    @pl.when(dp == 0)
    def _():
        pl.semaphore_wait(know.at[0], 1)

    @pl.when(dp == ndp - 1)
    def _():
        pl.semaphore_wait(know.at[1], 1)


def pass_word(ndp, know, ends):
    dp = lax.axis_index("dp")

    def tell(side, target):
        pl.semaphore_signal(
            know.at[side], inc=1, device_id={"dp": target}, device_id_type=pl.DeviceIdType.MESH
        )

    @pl.when(jnp.logical_and(dp > 0, dp < ndp - 1))
    def _():
        tell(0, dp - 1)
        tell(1, dp + 1)

    for t in range(ndp - 2):
        if not ends:
            @pl.when(jnp.logical_and(dp > 0, dp < ndp - 2 - t))
            def _():
                pl.semaphore_wait(know.at[0], 1)
                tell(0, dp - 1)

            @pl.when(jnp.logical_and(dp > 1 + t, dp < ndp - 1))
            def _():
                pl.semaphore_wait(know.at[1], 1)
                tell(1, dp + 1)

            continue

        @pl.when(dp < ndp - 2 - t)
        def _():
            pl.semaphore_wait(know.at[0], 1)

            @pl.when(dp > 0)
            def _():
                tell(0, dp - 1)

        @pl.when(dp > 1 + t)
        def _():
            pl.semaphore_wait(know.at[1], 1)

            @pl.when(dp < ndp - 1)
            def _():
                tell(1, dp + 1)


def silu(v):
    return v / (1.0 + jnp.exp(-v))


def softplus(v):
    return jnp.maximum(v, 0.0) + jnp.log1p(jnp.exp(-jnp.abs(v)))


def expand(per_head, at, rows):
    per = LANES // HEAD_DIM
    lane = lax.broadcasted_iota(jnp.int32, (rows, LANES), 1)
    out = jnp.broadcast_to(per_head[:, at : at + 1], (rows, LANES))
    for j in range(1, per):
        other = jnp.broadcast_to(per_head[:, at + j : at + j + 1], (rows, LANES))
        out = jnp.where(lane >= j * HEAD_DIM, other, out)
    return out


SEND_KINDS = ("x", "a", "b", "p", "n", "o", "f", "e", "q")


def far_first(me, n):
    low = jnp.asarray(me < (n + 1) // 2, jnp.int32)
    out = []
    for j in range(n - 1):
        up = j + jnp.asarray(j >= me, jnp.int32)
        down = n - 1 - (j + jnp.asarray(j >= n - 1 - me, jnp.int32))
        out.append(low * down + (1 - low) * up)
    return out


def settle(ref, sem):
    pltpu.make_async_copy(ref, ref, sem).wait()


def mixer_kernel(ntp, ndp, names, *refs):
    s = types.SimpleNamespace(**dict(zip(names, refs)))
    rows_t, width = s.tokens.shape
    batch = rows_t * ntp
    rows_d = batch // ndp
    cols = s.w_in.shape[3]
    vcols = s.w_vec.shape[3]
    heads = s.w_step.shape[2]
    local_heads = s.ssm.shape[2]
    groups = vcols // STATE_DIM
    span = cols // groups
    group_heads = local_heads // groups
    block = s.send_p.shape[4]
    blocks = cols // block
    tp = lax.axis_index("tp")
    dp = lax.axis_index("dp")
    core = lax.rem(tp, 2)
    partner = tp + 1 - 2 * core
    far = far_first(dp, ndp)
    relay = ndp == 4
    at_end = jnp.logical_or(dp == 0, dp == ndp - 1)
    inside = jnp.logical_not(at_end)
    across = ndp - 1 - dp

    def load(src, dst, sem):
        copy = pltpu.make_async_copy(src, dst, sem)
        copy.start()
        return copy

    def load_weights(layer):
        vec = [
            load(s.w_vec_hbm.at[layer, role], s.w_vec.at[layer, role], s.weight_sem.at[role])
            for role in (1, 0)
        ]
        step = load(s.w_step_hbm.at[layer], s.w_step.at[layer], s.weight_sem.at[2])
        return vec, step, [
            load(s.w_in_hbm.at[layer, role], s.w_in.at[layer, role], s.weight_sem.at[3 + role])
            for role in (1, 0)
        ]

    def load_rest(layer):
        return (
            load(s.ssm_hbm.at[layer], s.ssm.at[layer], s.rest_sem.at[layer, 0]),
            load(s.w_out_hbm.at[layer], s.w_out.at[layer], s.rest_sem.at[layer, 1]),
        )

    barrier, callers = call_out(ntp, ndp)
    own = load(s.x_hbm, s.landed.at[tp], s.own_sem.at[0])
    smalls = [load(s.gain_hbm, s.gain, s.small_sem.at[0])]
    own.wait()
    weights = [load_weights(0)]
    smalls += [
        load(getattr(s, name + "_hbm"), getattr(s, name), s.small_sem.at[i])
        for i, name in enumerate(SMALLS) if i
    ]
    pl.semaphore_wait(barrier, callers)
    for k in range(1, ntp):
        remote(
            s.landed.at[tp], s.landed.at[tp], s.sent.at[0], s.got_x.at[0],
            "tp", lax.rem(tp + k, ntp),
        ).start()
    s.drive_pad[...] = jnp.zeros_like(s.drive_pad)
    s.decay_pad[...] = jnp.zeros_like(s.decay_pad)
    s.outer[...] = jnp.zeros_like(s.outer)
    if relay:
        @pl.when(at_end)
        def _():
            for layer in range(LAYER_COUNT):
                for c in range(2 * blocks - 1):
                    s.land_p[layer, c, across] = jnp.zeros((rows_d, block), BF16)

    pass_word(ndp, s.know, not relay)
    smalls[0].wait()
    settle(s.landed.at[pl.ds(0, ntp - 1)], s.got_x.at[0])
    rest = [load_rest(0)]

    def send_part(layer, c, peer):
        remote(
            s.send_p.at[layer, c, peer], s.land_p.at[layer, c, dp],
            s.sent.at[SEND_KINDS.index("p")], s.got_p.at[layer, c], "dp", peer,
        ).start()

    near = jnp.where(dp == 0, 1, ndp - 2)
    middle = ndp - 1 - near
    side = (dp - 1) * 3

    def deal_relayed(layer, c):
        final = c == 2 * blocks - 1

        @pl.when(at_end)
        def _():
            if not final:
                remote(
                    s.send_p.at[layer, c, across], s.land_r.at[layer, c],
                    s.sent.at[SEND_KINDS.index("p")], s.got_r.at[layer, c], "dp", near,
                ).start()
            else:
                for e in range(c):
                    send_part(layer, e, middle)
                send_part(layer, c, across)
                send_part(layer, c, middle)
                for e in range(c + 1):
                    send_part(layer, e, near)

        @pl.when(inside)
        def _():
            send_part(layer, c, side)
            if not final:
                send_part(layer, c, across)
            else:
                other = 3 - side
                for e in range(c):
                    settle(s.land_r.at[layer, e], s.got_r.at[layer, e])
                    s.send_p[layer, e, other] = (
                        s.send_p[layer, e, other].astype(F32) + s.land_r[layer, e].astype(F32)
                    ).astype(BF16)
                    send_part(layer, e, other)
                send_part(layer, c, other)
                send_part(layer, c, across)

    def project(layer, rows):
        scale_row = s.gain[...].astype(F32)[layer : layer + 1]
        squares = []
        for i in range(ntp):
            part = rows(i)
            squares.append(jnp.sum(part * part, axis=1, keepdims=True))
            s.lhs_buf[i * rows_t : (i + 1) * rows_t, :] = part * scale_row
        squares = jnp.concatenate(squares, axis=0)
        lhs = s.lhs_buf[...].astype(BF16)
        load_vec, load_step, load_in = weights[layer]

        def put(target, at, acc):
            for p in range(ndp):
                target[p, :, at : at + acc.shape[1]] = acc[p * rows_d : (p + 1) * rows_d].astype(
                    BF16
                )

        def deal(target, landing, kind, got, peers=far):
            for peer in peers:
                remote(
                    target.at[peer], landing.at[dp], s.sent.at[SEND_KINDS.index(kind)], got,
                    "dp", peer,
                ).start()

        def deal_small(kind, target, landing, got):
            args = (target.at[layer], landing.at[layer], kind, got.at[layer])
            if relay:
                @pl.when(at_end)
                def _():
                    deal(*args, (middle,) if layer == 0 else (across, middle))

                @pl.when(inside)
                def _():
                    deal(*args)
            else:
                deal(*args)
            return args

        load_vec[0].wait()
        put(s.send_a.at[layer], 0, jnp.dot(lhs, s.w_vec[layer, 1], preferred_element_type=F32))
        if relay and layer == 0:
            learn_one(ndp, s.know)
        late = [deal_small("a", s.send_a, s.land_a, s.got_a)]
        load_step.wait()
        load_vec[1].wait()
        small = jnp.dot(lhs, s.w_step[layer], preferred_element_type=F32)
        small = pltpu.roll(small, lax.rem(heads - tp * local_heads, heads), 1)
        lane = lax.broadcasted_iota(jnp.int32, small.shape, 1)
        small = jnp.where(lane == local_heads, jnp.broadcast_to(squares, small.shape), small)
        put(s.send_b.at[layer], vcols, small)
        put(s.send_b.at[layer], 0, jnp.dot(lhs, s.w_vec[layer, 0], preferred_element_type=F32))
        late.append(deal_small("b", s.send_b, s.land_b, s.got_b))
        for j, role in enumerate((1, 0)):
            load_in[j].wait()
            for b in range(blocks):
                c = j * blocks + b
                acc = jnp.dot(
                    lhs, s.w_in[layer, role, :, b * block : (b + 1) * block],
                    preferred_element_type=F32,
                )
                put(s.send_p.at[layer, c], 0, acc)
                if relay:
                    deal_relayed(layer, c)
                    if layer == 0 and c == blocks - 1:
                        learn_one(ndp, s.know)

                        @pl.when(at_end)
                        def _():
                            for args in late:
                                deal(*args, (across,))

                    if c == 2 * blocks - 2:
                        @pl.when(at_end)
                        def _():
                            for args in late:
                                deal(*args, (near,))

                else:
                    deal(s.send_p.at[layer, c], s.land_p.at[layer, c], "p", s.got_p.at[layer, c])

    def total(mine, others):
        acc = mine[dp].astype(F32)
        for k in range(1, ndp):
            acc = acc + others[lax.rem(dp + k, ndp)].astype(F32)
        return acc

    def arrived(landing, got):
        settle(landing.at[pl.ds(0, ndp - 1)], got)

    def arrived_part(layer, c):
        if relay and c < 2 * blocks - 1:
            @pl.when(at_end)
            def _():
                settle(s.land_p.at[layer, c, pl.ds(0, ndp - 2)], s.got_p.at[layer, c])

            @pl.when(inside)
            def _():
                settle(s.land_p.at[layer, c, pl.ds(0, ndp - 1)], s.got_p.at[layer, c])
        else:
            arrived(s.land_p.at[layer, c], s.got_p.at[layer, c])

    def head_step(layer):
        if layer == 0:
            for copy in smalls[1:]:
                copy.wait()
        arrived(s.land_a.at[layer], s.got_a.at[layer])
        arrived(s.land_b.at[layer], s.got_b.at[layer])
        small = total(s.send_b.at[layer], s.land_b.at[layer])
        own_sq = small[:, vcols + local_heads : vcols + local_heads + 1]
        scale = lax.rsqrt(own_sq * (1.0 / MODEL_WIDTH) + EPS)
        taps_v = s.conv_v[layer].astype(F32)
        acts = []
        for role in range(2):
            raw = small[:, 0:vcols] if role == 0 else total(s.send_a.at[layer], s.land_a.at[layer])
            fresh = (raw * scale).astype(BF16)
            acc = fresh.astype(F32) * taps_v[role, 3:4]
            for i in range(3):
                acc = acc + s.vec_s[layer, role, i].astype(F32) * taps_v[role, i : i + 1]
            s.new_vec[layer, role, 0] = s.vec_s[layer, role, 1]
            s.new_vec[layer, role, 1] = s.vec_s[layer, role, 2]
            s.new_vec[layer, role, 2] = fresh
            acts.append(silu(acc))
        in_vec, out_vec = acts
        step = softplus(
            small[:, vcols : vcols + local_heads] * scale + s.bias[layer : layer + 1]
        )
        decay = jnp.exp(-step * jnp.exp(s.decay_log[layer : layer + 1]))
        s.decay_pad[0:rows_d, 0:local_heads] = decay
        s.decay_t[...] = jnp.transpose(s.decay_pad[...])
        rest[layer][0].wait()
        row = lax.broadcasted_iota(jnp.int32, (rows_d, STATE_DIM), 0)
        skips = jnp.broadcast_to(s.skip[layer : layer + 1], (rows_d, local_heads))
        inner = []
        for g in range(groups):
            in_g = in_vec[:, g * STATE_DIM : (g + 1) * STATE_DIM]
            out_g = out_vec[:, g * STATE_DIM : (g + 1) * STATE_DIM]
            inner.append(jnp.sum(in_g * out_g, axis=1, keepdims=True))
            acc = jnp.zeros((rows_d, span), F32)
            for r in range(rows_d):
                mine = jnp.where(row == r, out_g, 0.0)
                state = s.ssm[layer, r, g * group_heads : (g + 1) * group_heads]
                acc = acc + lax.dot_general(
                    mine, state.reshape(span, STATE_DIM), (((1,), (1,)), ((), ())),
                    preferred_element_type=F32,
                )
            s.read[:, g * span : (g + 1) * span] = acc
            high = in_g.astype(BF16).astype(F32)
            for r in range(rows_d):
                at = (r % 2) * STATE_DIM
                lanes = slice(at, at + STATE_DIM)
                mine = jnp.where(row == r, high, 0.0)
                s.outer[g, r // 2, 0:rows_d, lanes] = mine
                s.outer[g, r // 2, rows_d : 2 * rows_d, lanes] = mine
                s.outer[g, r // 2, 2 * rows_d : 3 * rows_d, lanes] = jnp.where(
                    row == r, in_g - high, 0.0
                )
        taps = s.conv_w[layer].astype(F32)
        for b in range(blocks):
            arrived_part(layer, b)
            cut = slice(b * block, (b + 1) * block)
            fresh = (total(s.send_p.at[layer, b], s.land_p.at[layer, b]) * scale).astype(BF16)
            acc = fresh.astype(F32) * taps[3:4, cut]
            for i in range(3):
                acc = acc + s.conv_s[layer, i, :, cut].astype(F32) * taps[i : i + 1, cut]
            s.new_conv[layer, 0, :, cut] = s.conv_s[layer, 1, :, cut]
            s.new_conv[layer, 1, :, cut] = s.conv_s[layer, 2, :, cut]
            s.new_conv[layer, 2, :, cut] = fresh
            values = silu(acc)
            for at in range(0, block, LANES):
                lane0 = b * block + at
                head = lane0 // HEAD_DIM
                v = values[:, at : at + LANES]
                drive = expand(step, head, rows_d) * v
                lanes = slice(lane0, lane0 + LANES)
                high = drive.astype(BF16).astype(F32)
                s.drive_pad[0:rows_d, lanes] = high
                s.drive_pad[rows_d : 2 * rows_d, lanes] = drive - high
                s.drive_pad[2 * rows_d : 3 * rows_d, lanes] = high
                s.read[:, lanes] = (
                    expand(decay, head, rows_d) * s.read[:, lanes]
                    + drive * inner[lane0 // span]
                    + expand(skips, head, rows_d) * v
                )
        gain_row = s.out_gain[...].astype(F32)[layer : layer + 1]
        for b in range(blocks):
            c = blocks + b
            arrived_part(layer, c)
            fresh = (total(s.send_p.at[layer, c], s.land_p.at[layer, c]) * scale).astype(BF16)
            mixed = s.read[:, b * block : (b + 1) * block] * silu(fresh.astype(F32))
            for at in range(0, block, span):
                cut = slice(b * block + at, b * block + at + span)
                part = mixed[:, at : at + span]
                mean = jnp.mean(part * part, axis=1, keepdims=True)
                s.held[layer, dp, :, cut] = (
                    part * lax.rsqrt(mean + EPS) * gain_row[:, cut]
                ).astype(BF16)
                g = (b * block + at) // span
                mine = s.held.at[layer, dp, :, pl.ds(g * span, span)]
                for peer in far:
                    remote(
                        mine, mine, s.sent.at[SEND_KINDS.index("n")], s.got_n.at[layer, g],
                        "dp", peer,
                    ).start()

    def update_state(layer, half):
        some = min(4, group_heads)
        for at in range(half * cols // 2, (half + 1) * cols // 2, LANES):
            s.drive_t[at : at + LANES, :] = jnp.transpose(s.drive_pad[:, at : at + LANES])

        def some_heads(q, carry):
            first = q * some
            lhs = s.drive_t[pl.ds(pl.multiple_of(first * HEAD_DIM, HEAD_DIM), some * HEAD_DIM), :]
            for pair in range(rows_d // 2):
                added = jnp.dot(
                    lhs, s.outer[first // group_heads, pair], preferred_element_type=F32
                )
                for r in (2 * pair, 2 * pair + 1):
                    at = (r % 2) * STATE_DIM
                    for j in range(some):
                        decay = s.decay_t[pl.ds(first + j, 1), :][:, r : r + 1]
                        s.ssm[layer, r, first + j] = (
                            s.ssm[layer, r, first + j]
                            * jnp.broadcast_to(decay, (HEAD_DIM, STATE_DIM))
                            + added[j * HEAD_DIM : (j + 1) * HEAD_DIM, at : at + STATE_DIM]
                        )
            return carry

        steps = local_heads // some
        lax.fori_loop(half * steps // 2, (half + 1) * steps // 2, some_heads, 0)

    def gather_out(layer, emit):
        rest[layer][1].wait()
        half = width // 2
        accs = [jnp.zeros((batch, half), F32)] * 2
        for g in range(groups):
            cut = slice(g * span, (g + 1) * span)
            settle(s.held.at[layer, pl.ds(0, ndp - 1), :, pl.ds(g * span, span)], s.got_n.at[layer, g])
            for i in range(ndp):
                s.lhs_out[i * rows_d : (i + 1) * rows_d, cut] = s.held[layer, i, :, cut].astype(F32)
            lhs = s.lhs_out[:, cut].astype(BF16)
            for h in range(2):
                accs[h] = accs[h] + jnp.dot(
                    lhs, s.w_out[layer, cut, h * half : (h + 1) * half], preferred_element_type=F32
                )
                if g == groups - 1:
                    emit(h, accs[h])

    project(0, lambda i: s.landed[i].astype(F32))
    for layer in range(LAYER_COUNT):
        last = layer == LAYER_COUNT - 1
        if not last:
            weights.append(load_weights(layer + 1))
            rest.append(load_rest(layer + 1))
        head_step(layer)
        update_state(layer, 0)
        half = width // 2

        def emit(h, acc, layer=layer, last=last):
            kind = s.sent.at[SEND_KINDS.index("f" if last else "o")]
            got = s.got_f.at[h] if last else s.got_o.at[layer]
            if last:
                for i in range(ntp):
                    s.send_f[h, i] = acc[i * rows_t : (i + 1) * rows_t].astype(BF16)
            elif h == 0:
                s.parts[layer, tp] = acc.astype(BF16)
            else:
                for q in range(2):
                    s.pair_out[layer, q] = acc[:, q * half // 2 : (q + 1) * half // 2].astype(BF16)
                remote(
                    s.pair_out.at[layer, 1 - core], s.pair_in.at[layer],
                    s.sent.at[SEND_KINDS.index("e")], s.got_e.at[layer], "tp", partner,
                ).start()
                return
            for k in range(1, ntp):
                peer = lax.rem(tp + k, ntp)
                src = s.send_f.at[h, peer] if last else s.parts.at[layer, tp]
                dst = s.land_f.at[h, tp] if last else src
                remote(src, dst, kind, got, "tp", peer).start()

        gather_out(layer, emit)
        if not last:
            settle(s.pair_in.at[layer], s.got_e.at[layer])
            s.quarters[layer, tp] = (
                s.pair_out[layer, core].astype(F32) + s.pair_in[layer].astype(F32)
            ).astype(BF16)
            for k in range(1, ntp):
                remote(
                    s.quarters.at[layer, tp], s.quarters.at[layer, tp],
                    s.sent.at[SEND_KINDS.index("q")], s.got_q.at[layer],
                    "tp", lax.rem(tp + k, ntp),
                ).start()
        update_state(layer, 1)
        if last:
            for h in range(2):
                cut = slice(h * half, (h + 1) * half)
                settle(s.land_f.at[h, pl.ds(0, ntp - 1)], s.got_f.at[h])
                s.land_f[h, tp] = s.send_f[h, tp]
                acc = s.rows[tp, :, cut].astype(F32)
                for i in range(ntp):
                    acc = acc + s.land_f[h, i].astype(F32)
                s.tokens[:, cut] = acc.astype(BF16)
        else:
            settle(s.parts.at[layer, pl.ds(0, ntp - 1)], s.got_o.at[layer])
            acc = s.parts[layer, 0].astype(F32)
            for i in range(1, ntp):
                acc = acc + s.parts[layer, i].astype(F32)
            accs = [acc]
            settle(s.quarters.at[layer, pl.ds(0, ntp - 1)], s.got_q.at[layer])
            for q in range(2):
                acc = s.quarters[layer, q].astype(F32)
                for i in range(q + 2, ntp, 2):
                    acc = acc + s.quarters[layer, i].astype(F32)
                accs.append(acc)
            acc = jnp.concatenate(accs, axis=1)
            before = s.landed if layer == 0 else s.rows

            def rows(i, before=before, acc=acc):
                part = (before[i].astype(F32) + acc[i * rows_t : (i + 1) * rows_t]).astype(BF16)
                s.rows[i] = part
                return part.astype(F32)

            project(layer + 1, rows)
    settle(s.landed.at[pl.ds(0, ntp - 1)], s.sent.at[0])
    settle(s.send_a.at[:, pl.ds(0, ndp - 1)], s.sent.at[1])
    settle(s.send_b.at[:, pl.ds(0, ndp - 1)], s.sent.at[2])
    settle(s.send_p.at[:, :, pl.ds(0, ndp - 1)], s.sent.at[3])
    settle(s.held.at[:, pl.ds(0, ndp - 1)], s.sent.at[4])
    settle(s.parts.at[:, pl.ds(0, ntp - 1)], s.sent.at[5])
    settle(s.pair_in, s.sent.at[7])
    settle(s.quarters.at[:, pl.ds(0, ntp - 1)], s.sent.at[8])
    settle(s.land_f.at[:, pl.ds(0, ntp - 1)], s.sent.at[6])


def write_kernel(tok, conv, vec, ssm, tok_out, conv_out, vec_out, ssm_out, sem, ssm_sem):
    layers, rows = ssm.shape[:2]
    for l in range(layers):
        for r in range(rows):
            pltpu.make_async_copy(ssm.at[l, r], ssm_out.at[l, r], ssm_sem).start()
    others = []
    for i, (src, dst) in enumerate(((tok, tok_out), (conv, conv_out), (vec, vec_out))):
        others.append(pltpu.make_async_copy(src, dst, sem.at[i]))
        others[-1].start()
    for copy in others:
        copy.wait()
    pltpu.make_async_copy(ssm, ssm_out, ssm_sem).wait()


VMEM = pl.BlockSpec(memory_space=pltpu.VMEM)
HBM = pl.BlockSpec(memory_space=pl.ANY)


def dma(*shape):
    return pltpu.SemaphoreType.DMA(shape)


SMALLS = (
    "gain", "conv_w", "conv_v", "conv_s", "vec_s", "bias", "decay_log", "skip", "out_gain"
)
INPUTS = ("x_hbm", "w_step_hbm", "w_in_hbm", "w_vec_hbm", "w_out_hbm", "ssm_hbm") + tuple(
    name + "_hbm" for name in SMALLS
)
SCRATCH = (
    "w_step", "w_in", "w_vec", "w_out",
) + SMALLS + (
    "landed", "lhs_buf", "send_a", "land_a", "send_b", "land_b", "send_p", "land_p",
    "read", "drive_pad", "drive_t", "outer", "decay_pad", "decay_t",
    "held", "lhs_out", "parts", "pair_out", "pair_in", "quarters", "rows", "send_f", "land_f", "land_r",
    "small_sem", "weight_sem", "rest_sem", "own_sem", "know", "sent", "got_x", "got_a", "got_b", "got_p", "got_r",
    "got_n", "got_o", "got_f", "got_e", "got_q",
)


def shards(
    ntp, ndp, tokens, w_in, w_vec, w_step, conv_weight, conv_vec, conv_state, vec_state,
    ssm_state, step_bias, decay_log, skip_gain, mix_gain, out_gain, w_out,
):
    rows_t, width = tokens.shape
    layers = w_in.shape[0]
    batch = rows_t * ntp
    rows_d = batch // ndp
    cols, vcols = w_in.shape[3], w_vec.shape[3]
    groups = vcols // STATE_DIM
    block = min(cols, 1024)
    chunks = 2 * cols // block
    conv_rows = jnp.transpose(conv_state, (0, 2, 1, 3))
    vec_rows = jnp.transpose(vec_state, (0, 1, 3, 2, 4))
    smalls = (
        mix_gain, conv_weight, conv_vec, conv_rows, vec_rows, step_bias, decay_log, skip_gain,
        out_gain,
    )
    scratch = [pltpu.VMEM(a.shape, a.dtype) for a in (w_step, w_in, w_vec, w_out) + smalls] + [
        pltpu.VMEM((ntp, rows_t, width), BF16),
        pltpu.VMEM((batch, width), F32),
        pltpu.VMEM((layers, ndp, rows_d, vcols), BF16),
        pltpu.VMEM((layers, ndp, rows_d, vcols), BF16),
        pltpu.VMEM((layers, ndp, rows_d, vcols + LANES), BF16),
        pltpu.VMEM((layers, ndp, rows_d, vcols + LANES), BF16),
        pltpu.VMEM((layers, chunks, ndp, rows_d, block), BF16),
        pltpu.VMEM((layers, chunks, ndp, rows_d, block), BF16),
        pltpu.VMEM((rows_d, cols), F32),
        pltpu.VMEM((LANES, cols), F32),
        pltpu.VMEM((cols, LANES), F32),
        pltpu.VMEM((groups, rows_d // 2, LANES, 2 * STATE_DIM), F32),
        pltpu.VMEM((LANES, LANES), F32),
        pltpu.VMEM((LANES, LANES), F32),
        pltpu.VMEM((layers, ndp, rows_d, cols), BF16),
        pltpu.VMEM((batch, cols), F32),
        pltpu.VMEM((layers - 1, ntp, batch, width // 2), BF16),
        pltpu.VMEM((layers - 1, 2, batch, width // 4), BF16),
        pltpu.VMEM((layers - 1, batch, width // 4), BF16),
        pltpu.VMEM((layers - 1, ntp, batch, width // 4), BF16),
        pltpu.VMEM((ntp, rows_t, width), BF16),
        pltpu.VMEM((2, ntp, rows_t, width // 2), BF16),
        pltpu.VMEM((2, ntp, rows_t, width // 2), BF16),
        pltpu.VMEM((layers, chunks - 1, rows_d, block), BF16),
        dma(len(SMALLS)), dma(5), dma(layers, 2), dma(1),
        pltpu.SemaphoreType.REGULAR((2,)), dma(len(SEND_KINDS)), dma(1), dma(layers),
        dma(layers), dma(layers, chunks), dma(layers, chunks - 1), dma(layers, groups),
        dma(layers - 1), dma(2), dma(layers - 1), dma(layers - 1),
    ]
    out_shape = (
        pltpu.VMEM(tokens.shape, BF16),
        pltpu.VMEM(conv_rows.shape, BF16),
        pltpu.VMEM(vec_rows.shape, BF16),
        pltpu.VMEM(ssm_state.shape, F32),
    )
    names = INPUTS + ("tokens", "new_conv", "new_vec", "ssm") + SCRATCH
    results = pl.pallas_call(
        functools.partial(mixer_kernel, ntp, ndp, names),
        out_shape=out_shape,
        in_specs=[HBM] * len(INPUTS),
        out_specs=(VMEM,) * len(out_shape),
        scratch_shapes=scratch,
        compiler_params=pltpu.CompilerParams(
            collective_id=0, has_side_effects=True, vmem_limit_bytes=44 << 20
        ),
    )(tokens, w_step, w_in, w_vec, w_out, ssm_state, *smalls)
    new_tokens, new_conv, new_vec, new_ssm = pl.pallas_call(
        write_kernel,
        out_shape=tuple(jax.ShapeDtypeStruct(r.shape, r.dtype) for r in results),
        in_specs=[VMEM] * 4,
        out_specs=(HBM,) * 4,
        scratch_shapes=[dma(3), pltpu.SemaphoreType.DMA],
        compiler_params=pltpu.CompilerParams(vmem_limit_bytes=8 << 20),
    )(*results)
    return (
        new_tokens,
        jnp.transpose(new_conv, (0, 2, 1, 3)),
        jnp.transpose(new_vec, (0, 1, 3, 2, 4)),
        new_ssm,
    )


def solution(mesh):
    placed = (
        P(("grp", "tp"), "dp"),
        P(None, None, "dp", "tp"),
        P(None, None, "dp", "tp"),
        P(None, "dp", None),
        P(None, None, "tp"),
        P(None, None, None, "tp"),
        P(None, ("grp", "dp"), None, "tp"),
        P(None, None, ("grp", "dp"), None, "tp"),
        P(None, ("grp", "dp"), "tp", None, None),
        P(None, "tp"),
        P(None, "tp"),
        P(None, "tp"),
        P(None, "dp"),
        P(None, "tp"),
        P(None, "tp", "dp"),
    )
    return jax.shard_map(
        functools.partial(shards, mesh.shape["tp"], mesh.shape["dp"]),
        mesh=mesh,
        in_specs=placed,
        out_specs=(
            P(("grp", "tp"), "dp"),
            P(None, ("grp", "dp"), None, "tp"),
            P(None, None, ("grp", "dp"), None, "tp"),
            P(None, ("grp", "dp"), "tp", None, None),
        ),
        check_vma=False,
    )
```
